32 devices in a mesh: ep: 8 (over z, x), tp: 4 (over y, core).
Axes of the slice: x: 2, y: 2, z: 4, core: 2. Of those that a mesh axis runs over, the one named last changes fastest.
Arguments:
- queries: bfloat16 [1024, 4096], P('ep', 'tp'), may hold values from -112 to 112
- key_rows: bfloat16 [1024, 4096], P('ep', 'tp'), may hold values from -8.1 to 8.1
- values: bfloat16 [1024, 4096], P('ep', 'tp'), may hold values from -6 to 6
- lambdas: float32 [16], P('tp'), may hold values from 0.3 to 0.8
- head_gain: float32 [256], replicated, may hold values from 0.1 to 1.9
- tokens: bfloat16 [512, 4096], P('ep'), may hold values from -6 to 6
- moe_gain: float32 [4096], replicated, may hold values from 0.1 to 1.9
- routes: int32 [512, 2], P('ep'), may hold values from 0 to 7, all different within a row; in each aligned block of 64 rows (0 to 63, 64 to 127, ...) at most 32 rows name the same one
- route_scores: float32 [512, 2], P('ep'), may hold values from -6 to 6
- w_gate: bfloat16 [8, 4096, 2048], P('ep', None, 'tp'), may hold values from -0.09375 to 0.09375
- w_up: bfloat16 [8, 4096, 2048], P('ep', None, 'tp'), may hold values from -0.09375 to 0.09375
- w_down: bfloat16 [8, 2048, 4096], P('ep', 'tp'), may hold values from -0.125 to 0.125
Outputs:
- attended: bfloat16 [1024, 4096], P('ep', 'tp')
- expert_out: bfloat16 [512, 4096], P('ep', 'tp')
The draws below stay inside these ranges and needn't reach their ends.
Inputs may be any that keep to these rules, and one draw needn't show every extreme that they name: `routes`: each row names 2 different experts. Among the rows of one index of ep at most 32 name the same expert, and some index reaches 32 in every draw.
All inputs are finite; a program needn't handle non-finite values.
Results may differ from the reference program's by a relative error of at most 0.018.
Values may be sent and summed in bfloat16 or wider, within the bound.
A program may use at most 64 MiB of HBM per device.

```python
import math
from functools import partial
import jax
import jax.numpy as jnp
import numpy as np
from jax import lax

D = 4096
HEADS = 16
QKD = 128
VD = 256
FF = 2048
TOP = 2
TOKB_DEV = 64
SEQ = 1024
TOKB = 512
EXPERTS = 8
CAP = 32
N_EP = 8
N_TP = 4


def base_pairs(key):
    seed_one, seed_two, seed_three, seed_four, seed_five = jax.random.split(jax.random.fold_in(key, 11), 5)
    row_width = HEADS * 2 * QKD
    queries = jnp.clip(jax.random.normal(seed_one, (SEQ, row_width), jnp.float32) * 1.3, -8.0, 8.0)
    key_rows = jnp.clip(jax.random.normal(seed_two, (SEQ, row_width), jnp.float32) * 1.3, -8.0, 8.0)
    return (queries, key_rows, seed_three, seed_four, seed_five)


def draw_queries(key, part):
    drawn = base_pairs(key)
    return drawn[0].astype(jnp.bfloat16)


def draw_key_rows(key, part):
    drawn = base_pairs(key)
    return drawn[1].astype(jnp.bfloat16)


def block_levels(own_key, shape, cuts, smallest, largest):
    gain = 1.0
    for dim, parts in cuts:
        heights = jax.random.uniform(jax.random.fold_in(jax.random.fold_in(own_key, 6), dim), (parts,), jnp.float32, smallest / len(cuts), largest / len(cuts))
        gain = gain * jnp.repeat(jnp.exp(heights), shape[dim] // parts).reshape((-1,) + (1,) * (len(shape) - 1 - dim))
    return gain


def shared_out(rng, own, number, rows, amount, top, reach, lean):
    ranking = jax.random.permutation(rng, amount)
    heavy_load, usual = shares(amount, rows * top, reach, lean, True), shares(amount, rows * top, reach, lean, False)
    places = jnp.arange(amount)

    def named(tallies, offset_by):
        used = int((tallies > 0).sum())
        fixed = max(1, used // 4)
        passed = fixed + (places - fixed + offset_by * (used - fixed)) % max(1, amount - fixed)
        return jnp.zeros((amount,), jnp.int32).at[ranking[jnp.where(places < fixed, places, passed)]].set(jnp.asarray(tallies, jnp.int32))

    tallies = jnp.where(number % 4 == 0, named(heavy_load, number // 4), named(usual, number - number // 4 - 1))
    mixed = jax.random.permutation(jax.random.fold_in(own, 3), amount)
    giver, sink = mixed[0:amount // 2 * 2:2], mixed[1:amount // 2 * 2:2]
    margin = jnp.minimum(tallies[giver] - 1, reach - tallies[sink]) // 2
    margin = jnp.where((giver == ranking[0]) | (sink == ranking[0]) | (tallies[sink] == 0), 0, jnp.maximum(margin, 0))
    passed = jax.random.randint(jax.random.fold_in(own, 4), (amount // 2,), 0, 1 << 20) % (margin + 1)
    tallies = tallies.at[giver].add(-passed).at[sink].add(passed)
    members = jnp.searchsorted(jnp.cumsum(tallies), jnp.arange(rows * top), side="right").astype(jnp.int32)
    grid = members.reshape(top, rows).T
    grid = grid[jax.random.permutation(jax.random.fold_in(own, 1), rows)]
    offset_by = jax.random.randint(jax.random.fold_in(own, 2), (rows, 1), 0, top)
    return jnp.take_along_axis(grid, (jnp.arange(top)[None, :] + offset_by) % top, axis=1)


def shares(number_of, total, reach, slope, full):
    loads = [(1 << 20) // math.isqrt(standing ** slope) + 1 for standing in range(1, number_of + 1)]
    largest = reach if full else min(reach, max(-(-total // number_of), total * loads[0] // sum(loads)))
    least = 1 if total - largest >= number_of - 1 else 0
    given, spare = [largest] + [least] * (number_of - 1), total - largest - least * (number_of - 1)
    while spare > 0:
        candidates = [i for i in range(1, number_of) if given[i] < largest] or [i for i in range(1, number_of) if given[i] < reach]
        whole, budget = sum([loads[i] for i in candidates]), spare
        for i in candidates:
            extra = min(reach - given[i], max(1, budget * loads[i] // whole), spare)
            given[i] = given[i] + extra
            spare = spare - extra
    return np.array(given)


def bell_draw(own_key, dims, spread, limit, pieces=(), held_as=jnp.bfloat16):
    array = spread * jax.random.normal(own_key, dims, jnp.float32)
    if pieces:
        array = array * block_levels(own_key, dims, pieces, -0.22, 0.18)
    return jnp.clip(array, -limit, limit).astype(held_as)


def setup_inputs(seed: int = 0) -> dict:
    arg_keys = jax.random.split(jax.random.key(seed), 13)
    queries = draw_queries(jax.random.fold_in(arg_keys[12], 71), 0)
    key_rows = draw_key_rows(jax.random.fold_in(arg_keys[12], 71), 0)
    values = bell_draw(arg_keys[2], (SEQ, HEADS * VD), 1.0, 6.0, ((0, 8), (1, 4)))
    lambdas = jnp.clip(0.3 + 0.5 * jax.random.uniform(arg_keys[3], (HEADS,), jnp.float32) ** block_levels(arg_keys[3], (HEADS,), ((0, 4),), -0.2, 0.2), 0.3, 0.8)
    head_gain = jnp.clip(1.0 + 0.18 * jax.random.normal(arg_keys[4], (VD,), jnp.float32), 0.1, 1.9)
    tokens = bell_draw(arg_keys[5], (TOKB, D), 1.0, 6.0, ((0, 8),))
    moe_gain = jnp.clip(1.0 + 0.18 * jax.random.normal(arg_keys[6], (D,), jnp.float32), 0.1, 1.9)
    routes_keys = jax.random.split(jax.random.fold_in(arg_keys[7], 1), TOKB // TOKB_DEV)
    routes_turns = jax.random.permutation(jax.random.fold_in(arg_keys[7], 3), TOKB // TOKB_DEV)
    routes = jax.vmap(lambda own, number: shared_out(jax.random.fold_in(arg_keys[7], 2), own, number, TOKB_DEV, EXPERTS, TOP, CAP, 1))(routes_keys, routes_turns).reshape((TOKB, TOP))
    route_scores = bell_draw(arg_keys[8], (TOKB, TOP), 1.0, 6.0, ((0, 8),), jnp.float32)
    w_gate = bell_draw(arg_keys[9], (EXPERTS, D, FF), D ** -0.5, 0.09375, ((0, 8), (2, 4)))
    w_up = bell_draw(arg_keys[10], (EXPERTS, D, FF), D ** -0.5, 0.09375, ((0, 8), (2, 4)))
    w_down = bell_draw(arg_keys[11], (EXPERTS, FF, D), FF ** -0.5, 0.125, ((0, 8), (1, 4)))
    return {"queries": queries, "key_rows": key_rows, "values": values, "lambdas": lambdas, "head_gain": head_gain, "tokens": tokens, "moe_gain": moe_gain, "routes": routes, "route_scores": route_scores, "w_gate": w_gate, "w_up": w_up, "w_down": w_down}


neg_big = -1e+30
head_eps = 1e-05
moe_eps = 1e-06
head_scale = 0.8

def slot_table(routes, experts, capacity):
    flat_routes = routes.reshape(-1)
    onehot = (flat_routes[:, None] == jnp.arange(experts, dtype=jnp.int32)[None, :]).astype(jnp.int32)
    before = jnp.cumsum(onehot, axis=0) - onehot
    position = lax.optimization_barrier(jnp.sum(before * onehot, axis=1))
    return (flat_routes * capacity + position).astype(jnp.int32).reshape(routes.shape)

def reference(queries, key_rows, values, lambdas, head_gain, tokens, moe_gain, routes, route_scores, w_gate, w_up, w_down):
    query_heads = queries.reshape(SEQ, HEADS, 2, QKD).transpose(1, 0, 2, 3)
    key_heads = key_rows.reshape(SEQ, HEADS, 2, QKD).transpose(1, 0, 2, 3)
    value_heads = values.reshape(SEQ, HEADS, VD).transpose(1, 0, 2)
    visible = jnp.tril(jnp.ones((SEQ, SEQ), dtype=bool))

    def one_head(inputs):
        query_h, key_h, value_h, weight_h = inputs
        scores = jnp.einsum('qmd,kmd->mqk', query_h.astype(jnp.float32), key_h.astype(jnp.float32), precision=lax.Precision.HIGHEST) * QKD ** (-0.5)
        scores = jnp.where(visible[None], scores, neg_big)
        probabilities = jax.nn.softmax(scores, axis=-1)
        mixing = probabilities[0] - weight_h * probabilities[1]
        mixed_out = jnp.dot(mixing, value_h.astype(jnp.float32), precision=lax.Precision.HIGHEST)
        scaled = mixed_out * lax.rsqrt(lax.optimization_barrier(jnp.mean(mixed_out * mixed_out, axis=-1, keepdims=True)) + head_eps)
        return (scaled * head_gain * head_scale).astype(jnp.bfloat16)
    heads_out = lax.map(one_head, (query_heads, key_heads, value_heads, lambdas))
    attended = heads_out.transpose(1, 0, 2).reshape(SEQ, HEADS * VD)
    token_f32 = tokens.astype(jnp.float32)
    normed = (token_f32 * lax.rsqrt(lax.optimization_barrier(jnp.mean(token_f32 * token_f32, axis=-1, keepdims=True)) + moe_eps) * moe_gain).astype(jnp.bfloat16)
    gate_weights = jax.nn.softmax(route_scores, axis=-1)
    local_slots = jax.vmap(partial(slot_table, experts=EXPERTS, capacity=CAP))(routes.reshape(N_EP, TOKB_DEV, TOP))
    expert_ids = local_slots // CAP
    within = local_slots % CAP
    source = jnp.arange(N_EP, dtype=jnp.int32)[:, None, None]
    global_slot = (expert_ids * (N_EP * CAP) + source * CAP + within).astype(jnp.int32).reshape(TOKB, TOP)
    row_ids = jnp.broadcast_to(jnp.arange(TOKB, dtype=jnp.int32)[:, None], (TOKB, TOP))
    row_of_slot = jnp.zeros((EXPERTS * N_EP * CAP,), jnp.int32).at[global_slot.reshape(-1)].set(row_ids.reshape(-1))
    gathered = normed[row_of_slot].reshape(EXPERTS, N_EP * CAP, D)
    group_size = FF // N_TP

    def one_expert(inputs):
        rows_e, gate_e, up_e, down_e = inputs
        gate_act = jnp.dot(rows_e, gate_e, preferred_element_type=jnp.float32)
        up_act = jnp.dot(rows_e, up_e, preferred_element_type=jnp.float32)
        hidden = (jax.nn.silu(gate_act) * up_act).astype(jnp.bfloat16)

        def add_group(group_index, running):
            offset = (group_index * group_size).astype(jnp.int32)
            hidden_part = lax.dynamic_slice_in_dim(hidden, offset, group_size, 1)
            down_part = lax.dynamic_slice_in_dim(down_e, offset, group_size, 0)
            partial_sum = jnp.dot(hidden_part, down_part, preferred_element_type=jnp.float32).astype(jnp.bfloat16)
            partial_sum = lax.optimization_barrier(partial_sum)
            return running + partial_sum.astype(jnp.float32)
        running = lax.fori_loop(jnp.int32(0), jnp.int32(N_TP), add_group, jnp.zeros((N_EP * CAP, D), jnp.float32))
        return running.astype(jnp.bfloat16)
    results = lax.map(one_expert, (gathered, w_gate, w_up, w_down)).reshape(EXPERTS * N_EP * CAP, D)
    picked = results[global_slot].astype(jnp.float32)
    expert_out = lax.optimization_barrier(jnp.sum(gate_weights[..., None] * picked, axis=1)).astype(jnp.bfloat16)
    return (attended, expert_out)
```

```python
import functools

import jax
import jax.numpy as jnp
from jax import lax
from jax.experimental import pallas as pl
from jax.experimental.pallas import tpu as pltpu
from jax.sharding import PartitionSpec as P

QKD = 128
VD = 256
TOP = 2


neg_big = -1e30
head_eps = 1e-05
moe_eps = 1e-06
head_scale = 0.8


def slot_table(routes, experts, capacity):
    flat_routes = routes.reshape(-1)
    onehot = (flat_routes[:, None] == jnp.arange(experts, dtype=jnp.int32)[None, :]).astype(
        jnp.int32
    )
    before = jnp.cumsum(onehot, axis=0) - onehot
    position = jnp.sum(before * onehot, axis=1)
    return (flat_routes * capacity + position).reshape(routes.shape)


def fold_block(state, query_group, query_pos, key_heads, value_heads, key_pos):
    maxima, denominators, accumulated = state
    scores = jnp.einsum(
        "qhmd,khmd->hmqk", query_group, key_heads, preferred_element_type=jnp.float32
    ) * QKD ** (-0.5)
    visible = key_pos[None, :] <= query_pos[:, None]
    scores = jnp.where(visible, scores, neg_big)
    new_max = jnp.maximum(maxima, jnp.max(scores, axis=-1))
    weights = jnp.where(visible, jnp.exp(scores - new_max[..., None]), 0.0)
    accumulated = jnp.einsum(
        "hmqk,khd->hmqd", weights, value_heads, precision=lax.Precision.HIGHEST
    )
    denominators = jnp.sum(weights, axis=-1)
    return (new_max, denominators, accumulated)


def local_general(
    queries,
    key_rows,
    values,
    lambdas,
    head_gain,
    tokens,
    moe_gain,
    routes,
    route_scores,
    w_gate,
    w_up,
    w_down,
):
    rows_a = queries.shape[0]
    half_rows = rows_a // 2
    head_local = lambdas.shape[0]
    ep_count = lax.axis_size("ep")
    ep_index = lax.axis_index("ep")
    early_queries = queries[:half_rows]
    later_queries = queries[half_rows:]
    early_pos = ep_index * rows_a + jnp.arange(half_rows, dtype=jnp.int32)
    later_pos = ep_index * rows_a + half_rows + jnp.arange(half_rows, dtype=jnp.int32)
    query_groups = (
        early_queries.reshape(half_rows, head_local, 2, QKD),
        later_queries.reshape(half_rows, head_local, 2, QKD),
    )
    position_groups = (early_pos, later_pos)
    start_state = (
        jnp.full((head_local, 2, half_rows), neg_big, jnp.float32),
        jnp.zeros((head_local, 2, half_rows), jnp.float32),
        jnp.zeros((head_local, 2, half_rows, VD), jnp.float32),
    )
    totals = (start_state, start_state)
    row_start = jnp.int32(0)
    key_block = lax.all_gather(key_rows, "ep", axis=0, tiled=True)
    value_block = lax.all_gather(values, "ep", axis=0, tiled=True)
    key_count = key_block.shape[0]
    key_heads = key_block.reshape(key_count, head_local, 2, QKD)
    value_heads = value_block.reshape(key_count, head_local, VD).astype(jnp.float32)
    key_pos = jnp.arange(key_count, dtype=jnp.int32)
    updated = []
    for attend_group_index in range(2):
        state = totals[attend_group_index]
        query_group = query_groups[attend_group_index]
        query_pos = position_groups[attend_group_index]
        state = lax.cond(
            row_start <= query_pos[-1],
            lambda held: fold_block(held, query_group, query_pos, key_heads, value_heads, key_pos),
            lambda held: held,
            state,
        )
        updated.append(state)
    folded = (updated[0], updated[1])
    attended_groups = []
    for group_index in range(2):
        maxima, denominators, accumulated = folded[group_index]
        mixed_out = (
            accumulated[:, 0] / denominators[:, 0, :, None]
            - lambdas[:, None, None] * accumulated[:, 1] / denominators[:, 1, :, None]
        )
        scaled = mixed_out * lax.rsqrt(
            jnp.mean(mixed_out * mixed_out, axis=-1, keepdims=True) + head_eps
        )
        scaled = scaled * head_gain * head_scale
        attended_groups.append(
            scaled.transpose(1, 0, 2).reshape(half_rows, head_local * VD).astype(jnp.bfloat16)
        )
    later_out = attended_groups[1]
    attended = jnp.concatenate([attended_groups[0], later_out], axis=0)
    rows_b = tokens.shape[0]
    capacity = 2 * TOP * rows_b // ep_count
    token_f32 = tokens.astype(jnp.float32)
    normed = (
        token_f32
        * lax.rsqrt(jnp.mean(token_f32 * token_f32, axis=-1, keepdims=True) + moe_eps)
        * moe_gain
    ).astype(jnp.bfloat16)
    gate_weights = jax.nn.softmax(route_scores, axis=-1)
    slot_of = slot_table(routes, ep_count, capacity)
    row_ids = jnp.broadcast_to(jnp.arange(rows_b, dtype=jnp.int32)[:, None], slot_of.shape)
    row_of_slot = (
        jnp.zeros((ep_count * capacity,), jnp.int32)
        .at[slot_of.reshape(-1)]
        .set(row_ids.reshape(-1))
    )
    gate_local = w_gate[0]
    up_local = w_up[0]
    down_local = w_down[0]
    outgoing = normed[row_of_slot]
    arrived = lax.all_to_all(outgoing, "ep", split_axis=0, concat_axis=0, tiled=True)
    gate_act = jnp.dot(arrived, gate_local, preferred_element_type=jnp.float32)
    up_act = jnp.dot(arrived, up_local, preferred_element_type=jnp.float32)
    hidden = (jax.nn.silu(gate_act) * up_act).astype(jnp.bfloat16)
    summed = lax.psum_scatter(
        lax.dot_general(
            down_local, hidden, (((0,), (1,)), ((), ())), preferred_element_type=jnp.float32
        ).astype(jnp.bfloat16),
        "tp",
        scatter_dimension=0,
        tiled=True,
    )
    returned = lax.all_to_all(summed, "ep", split_axis=1, concat_axis=1, tiled=True)
    slot_ids = jnp.arange(ep_count * capacity, dtype=jnp.int32)
    combined = jnp.zeros((rows_b, returned.shape[0]), jnp.float32)
    for choice_index in range(TOP):
        picker = (slot_of[:, choice_index, None] == slot_ids[None, :]).astype(jnp.bfloat16)
        picked = lax.dot_general(
            picker, returned, (((1,), (1,)), ((), ())), preferred_element_type=jnp.float32
        )
        combined = combined + gate_weights[:, choice_index, None] * picked
    expert_out = combined.astype(jnp.bfloat16)
    return (attended, expert_out)


MESH = pl.DeviceIdType.MESH


def step_kernel(
    n,
    heads,
    q_in,
    k_in,
    v_in,
    lam_ref,
    gain_ref,
    tokens_in,
    moe_gain_ref,
    routes_ref,
    score_ref,
    wg_ref,
    wu_ref,
    wd_ref,
    att_ref,
    out_ref,
    wg,
    wu,
    wd,
    qb,
    kb,
    vb,
    qm,
    pr,
    stat_out,
    stat_in,
    osend,
    oret,
    fin,
    att_in,
    routes_m,
    score_m,
    dense,
    dense_m,
    pick,
    tok,
    arr,
    part,
    near,
    csum,
    far,
    res,
    ret,
    back,
    back_m,
    q_ref,
    k_ref,
    v_ref,
    tokens_ref,
    w_sem,
    m_send,
    m_recv,
    tok_send,
    tok_recv,
    ty_send,
    ty_recv,
    tc_send,
    tc_recv,
    a_send,
    a_recv,
    qm_send,
    qm_recv,
    x_send,
    x_recv,
    f_send,
    f_recv,
    rc_send,
    rc_recv,
    ry_send,
    ry_recv,
    e_send,
    e_recv,
):
    me = lax.axis_index("ep")
    tp = lax.axis_index("tp")
    y = tp // 2
    core = tp % 2
    tp_core = y * 2 + 1 - core
    tp_y = (1 - y) * 2 + core
    tp_both = (1 - y) * 2 + 1 - core
    g = n // 2
    half = me // g
    w = me % g
    base = half * g
    mirror = (1 - half) * g + w
    rows = q_ref.shape[0]
    rows_b = tokens_ref.shape[0]
    slots, width = tok.shape[2:]
    total = g * slots

    def ahead(j):
        return lax.rem(w + j, g)

    def behind(j):
        return lax.rem(w + g - j, g)

    def remote(src, dst, send, recv, ep, tpi):
        return pltpu.make_async_remote_copy(
            src_ref=src,
            dst_ref=dst,
            send_sem=send,
            recv_sem=recv,
            device_id=(ep, tpi),
            device_id_type=MESH,
        )

    barrier = pltpu.get_barrier_semaphore()
    for j in range(1, g):
        pl.semaphore_signal(barrier, inc=1, device_id=(base + ahead(j), tp), device_id_type=MESH)
    pl.semaphore_signal(barrier, inc=1, device_id=(mirror, tp), device_id_type=MESH)
    pl.semaphore_signal(barrier, inc=1, device_id=(me, tp_core), device_id_type=MESH)
    pl.semaphore_signal(barrier, inc=1, device_id=(me, tp_y), device_id_type=MESH)
    staged = [
        pltpu.make_async_copy(src, dst, w_sem.at[3 + i])
        for i, (src, dst) in enumerate(
            ((tokens_in, tokens_ref), (q_in, q_ref), (k_in, k_ref), (v_in, v_ref))
        )
    ]
    for c in staged:
        c.start()
    loads = [
        pltpu.make_async_copy(wg_ref.at[0], wg, w_sem.at[0]),
        pltpu.make_async_copy(wu_ref.at[0], wu, w_sem.at[1]),
        pltpu.make_async_copy(wd_ref.at[0], wd, w_sem.at[2]),
    ]
    for load in loads:
        load.start()

    features = pl.ds(pl.multiple_of(tp * width, width), width)
    staged[0].wait()
    token_f32 = tokens_ref[...].astype(jnp.float32)
    inverse = lax.rsqrt(jnp.mean(token_f32 * token_f32, axis=-1, keepdims=True) + moe_eps)
    dense[...] = (
        tokens_ref[:, features].astype(jnp.float32) * inverse * moe_gain_ref[:, features]
    ).astype(jnp.bfloat16)
    lane = lax.broadcasted_iota(jnp.int32, (rows_b, 128), 1)
    square = (rows_b, rows_b)
    row_at = lax.broadcasted_iota(jnp.int32, square, 0)
    column_at = lax.broadcasted_iota(jnp.int32, square, 1)
    below = jnp.where(column_at < row_at, 1.0, 0.0).astype(jnp.bfloat16)
    slot_ids = lax.broadcasted_iota(jnp.int32, (rows_b, total), 1).astype(jnp.float32)

    def upright(ref, c):
        line = jnp.broadcast_to(ref[c : c + 1, :], square)
        return jnp.sum(
            jnp.where(row_at == column_at, line, jnp.zeros_like(line)), axis=1, keepdims=True
        )

    def choose(group, ref, source):
        named_by = [upright(ref, c) for c in range(TOP)]
        named = [named_by[c] == lane for c in range(TOP)]
        either = jnp.where(named[0] | named[1], 1.0, 0.0).astype(jnp.bfloat16)
        before = jnp.dot(below, either, preferred_element_type=jnp.float32)
        chosen = jnp.zeros((rows_b, total), jnp.float32)
        for c in range(TOP):
            position = jnp.sum(jnp.where(named[c], before, 0.0), axis=1, keepdims=True)
            slot = (named_by[c] - base).astype(jnp.float32) * slots + position
            hit = jnp.where(slot == slot_ids, 1.0, 0.0)
            pick[group, c] = hit.astype(jnp.bfloat16)
            chosen = chosen + hit
        tok[group] = (
            jnp.dot(
                chosen.T.astype(jnp.bfloat16), source[...], preferred_element_type=jnp.float32
            )
            .astype(jnp.bfloat16)
            .reshape(g, slots, width)
        )

    choose(0, routes_ref, dense)
    pl.semaphore_wait(barrier, g + 2)

    for c in staged[1:]:
        c.wait()
    sent = []
    mirrored = [
        remote(routes_ref, routes_m, m_send.at[0], m_recv.at[0], mirror, tp),
        remote(score_ref, score_m, m_send.at[1], m_recv.at[1], mirror, tp),
        remote(dense, dense_m, m_send.at[2], m_recv.at[2], mirror, tp),
    ]
    for c in mirrored:
        c.start()
    sent += mirrored
    tok_copies = {}

    def scatter(group):
        for j in range(1, g):
            d = ahead(j)
            c = remote(
                tok.at[group, d],
                arr.at[tp, group, w],
                tok_send.at[group, j],
                tok_recv.at[group, j],
                base + d,
                tp,
            )
            c.start()
            tok_copies[group, j] = c

    unit_copies = {}

    def share(which, src, dst):
        for j in range(1, g):
            d = ahead(j)
            cols = pl.ds(pl.multiple_of(d * VD, VD), VD)
            c = remote(
                src.at[:, cols],
                dst.at[w],
                a_send.at[which, j],
                a_recv.at[which, j],
                base + d,
                tp,
            )
            c.start()
            unit_copies[which, j] = c

    y_copies, core_copies, more_copies = {}, {}, {}

    def hand(group, j):
        s = behind(j)
        if j == 0:
            src = tok.at[group, w]
            arr[tp, group, w] = tok[group, w]
        else:
            tok_copies[group, j].wait_recv()
            src = arr.at[tp, group, s]
        c = remote(
            src, arr.at[tp, group, s], ty_send.at[group, j], ty_recv.at[group, j], me, tp_y
        )
        c.start()
        y_copies[group, j] = c
        c = remote(
            src,
            arr.at[tp, group, s],
            tc_send.at[0, group, j],
            tc_recv.at[0, group, j],
            me,
            tp_core,
        )
        c.start()
        core_copies[group, j] = c

    scatter(0)
    share(1, q_ref, qb)
    hand(0, 0)
    own = pl.ds(pl.multiple_of(w * VD, VD), VD)
    kb[w] = k_ref[:, own]
    qb[w] = q_ref[:, own]
    vb[w] = v_ref[:, own]
    for j in range(1, g):
        hand(0, j)
    for c in mirrored:
        c.wait_recv()
    choose(1, routes_m, dense_m)
    scatter(1)
    hand(1, 0)
    def q_on(s):
        return remote(qb.at[s], qm.at[s], qm_send.at[s], qm_recv.at[s], mirror, tp)

    @pl.when(half == 1)
    def _():
        for j in range(1, g):
            unit_copies[1, j].wait_recv()
        for s in range(g):
            q_on(s).start()

    share(0, k_ref, kb)
    share(2, v_ref, vb)

    def first_products(group, quarter):
        a = arr[quarter, group].reshape(total, width)
        deep = pl.ds(pl.multiple_of(quarter * width, width), width)
        return (
            jnp.dot(a, wg[deep, :], preferred_element_type=jnp.float32),
            jnp.dot(a, wu[deep, :], preferred_element_type=jnp.float32),
        )

    def near_half(group):
        one = first_products(group, tp)
        for j in range(g):
            core_copies[group, j].wait_recv()
        two = first_products(group, tp_core)
        return one[0] + two[0], one[1] + two[1]

    order = (tp_both, tp_y, tp_core, tp)
    near_copies, far_copies = {}, {}

    def far_half(group, gate, up):
        for j in range(g):
            s = behind(j)
            y_copies[group, j].wait_recv()
            c = remote(
                arr.at[tp_y, group, s],
                arr.at[tp_y, group, s],
                tc_send.at[1, group, j],
                tc_recv.at[1, group, j],
                me,
                tp_core,
            )
            c.start()
            more_copies[group, j] = c
        more = first_products(group, tp_y)
        gate, up = gate + more[0], up + more[1]
        for j in range(g):
            more_copies[group, j].wait_recv()
        more = first_products(group, tp_both)
        gate, up = gate + more[0], up + more[1]
        return (jax.nn.silu(gate) * up).astype(jnp.bfloat16)

    def second_products(group, hidden):
        for i in range(4):
            cols = pl.ds(pl.multiple_of(order[i] * width, width), width)
            part[group, i] = (
                jnp.dot(hidden, wd[:, cols], preferred_element_type=jnp.float32)
                .astype(jnp.bfloat16)
                .reshape(g, slots, width)
            )
            if i % 2 == 0:
                h = i // 2
                c = remote(
                    part.at[group, i],
                    near.at[group, h],
                    rc_send.at[group, h],
                    rc_recv.at[group, h],
                    me,
                    tp_core,
                )
                c.start()
                near_copies[group, h] = c
        near_copies[group, 0].wait_recv()
        for j in range(g):
            d = ahead(j)
            csum[group, d] = (
                part[group, 1, d].astype(jnp.float32) + near[group, 0, d].astype(jnp.float32)
            ).astype(jnp.bfloat16)
            c = remote(
                csum.at[group, d],
                far.at[group, d],
                ry_send.at[group, j],
                ry_recv.at[group, j],
                me,
                tp_y,
            )
            c.start()
            far_copies[group, j] = c

    back_copies = {}

    def expert_back(group):
        near_copies[group, 1].wait_recv()
        for j in range(g):
            d = ahead(j)
            far_copies[group, j].wait_recv()
            val = (
                part[group, 3, d].astype(jnp.float32)
                + near[group, 1, d].astype(jnp.float32)
                + far[group, d].astype(jnp.float32)
            ).astype(jnp.bfloat16)
            if j == 0:
                ret[group, w] = val
            else:
                res[group, d] = val
                c = remote(
                    res.at[group, d],
                    ret.at[group, w],
                    e_send.at[group, j],
                    e_recv.at[group, j],
                    base + d,
                    tp,
                )
                c.start()
                back_copies[group, j] = c

    def combine(group, ref):
        for j in range(1, g):
            back_copies[group, j].wait_recv()
        first, second = upright(ref, 0), upright(ref, 1)
        top = jnp.maximum(first, second)
        raised = (jnp.exp(first - top), jnp.exp(second - top))
        returned = ret[group].reshape(total, width)
        combined = jnp.zeros(out_ref.shape, jnp.float32)
        for c in range(TOP):
            picked = jnp.dot(pick[group, c], returned, preferred_element_type=jnp.float32)
            combined = combined + raised[c] / (raised[0] + raised[1]) * picked
        return combined

    loads[0].wait()
    loads[1].wait()
    gate, up = near_half(0)
    hidden = far_half(0, gate, up)
    for j in range(1, g):
        hand(1, j)
    loads[2].wait()
    second_products(0, hidden)
    lam = lam_ref[w]
    size = 2 * rows
    blocks = g // 2
    reach = g * rows
    diag = (
        lax.broadcasted_iota(jnp.int32, (size, size), 1)
        <= lax.broadcasted_iota(jnp.int32, (size, size), 0)
    )
    stat_lane = lax.broadcasted_iota(jnp.int32, (size, 128), 1)

    def weigh(q, seen, masked):
        found = []
        for m in range(2):
            cols = slice(m * QKD, (m + 1) * QKD)
            k = kb[0 : seen // rows].reshape(seen, 2 * QKD)[:, cols]
            scores = lax.dot_general(
                q[:, cols], k, (((1,), (1,)), ((), ())), preferred_element_type=jnp.float32
            ) * QKD ** (-0.5)
            if masked:
                last = jnp.where(diag, scores[:, seen - size :], neg_big)
                scores = (
                    last
                    if seen == size
                    else jnp.concatenate([scores[:, : seen - size], last], axis=1)
                )
            top = jnp.max(scores, axis=-1, keepdims=True)
            weights = jnp.exp(scores - top)
            found.append((weights, top, jnp.sum(weights, axis=-1, keepdims=True)))
        return found

    def blend(first, second, one, two, seen):
        v = vb[0 : seen // rows].reshape(seen, VD)
        mixed = (first * one - second * two).astype(jnp.bfloat16)
        return jnp.dot(mixed, v, preferred_element_type=jnp.float32)

    def keep(i, seen, found):
        (one, top_one, sum_one), (two, top_two, sum_two) = found
        line = pl.ds(i * size, size)
        pr[0, line, 0:seen] = one
        pr[1, line, 0:seen] = two
        packed = jnp.where(
            stat_lane == 0,
            top_one,
            jnp.where(stat_lane == 1, sum_one, jnp.where(stat_lane == 2, top_two, sum_two)),
        )
        stat_out[:, line] = packed.T[0:8]

    def stats_on():
        return remote(stat_out, stat_in, x_send.at[0], x_recv.at[0], mirror, tp)

    def o_on(i):
        line = pl.ds(i * size, size)
        return remote(
            osend.at[line], oret.at[line], x_send.at[1 + i], x_recv.at[1 + i], mirror, tp
        )

    def merged():
        mine, other = stat_out[...], stat_in[...]
        scale = []
        for m in range(2):
            top, bottom = mine[2 * m : 2 * m + 1], mine[2 * m + 1 : 2 * m + 2]
            top_o, bottom_o = other[2 * m : 2 * m + 1], other[2 * m + 1 : 2 * m + 2]
            high = jnp.maximum(top, top_o)
            part_mine = jnp.exp(top - high)
            scale.append(part_mine / (bottom * part_mine + bottom_o * jnp.exp(top_o - high)))
        at = lax.broadcasted_iota(jnp.int32, (128, reach), 0)
        both = jnp.where(at == 0, scale[0], jnp.where(at == 1, scale[1] * lam, 0.0))
        return both.T

    def f_on(d):
        return remote(fin.at[d], att_in.at[w], f_send.at[d], f_recv.at[w], base + d, tp)

    def finish(i, mixed):
        scaled = mixed * lax.rsqrt(jnp.mean(mixed * mixed, axis=-1, keepdims=True) + head_eps)
        scaled = (scaled * gain_ref[...] * head_scale).astype(jnp.bfloat16)
        fin[2 * i : 2 * i + 2] = scaled.reshape(2, rows, VD)
        for d in (2 * i, 2 * i + 1):

            @pl.when(d != w)
            def _(d=d):
                f_on(d).start()

            @pl.when(d == w)
            def _(d=d):
                att_in[w] = fin[d]

    gate, up = near_half(1)
    hidden = far_half(1, gate, up)
    second_products(1, hidden)

    for j in range(1, g):
        unit_copies[0, j].wait_recv()

    @pl.when(half == 1)
    def _():
        for i in range(blocks):
            q = qb[2 * i : 2 * i + 2].reshape(size, 2 * QKD)
            seen = (i + 1) * size
            keep(i, seen, weigh(q, seen, True))
        stats_on().start()

    @pl.when(half == 0)
    def _():
        for s in range(g):
            q_on(s).wait_recv()
        for i in range(blocks):
            q = qm[2 * i : 2 * i + 2].reshape(size, 2 * QKD)
            keep(i, reach, weigh(q, reach, False))
        stats_on().start()

    for j in range(1, g):
        unit_copies[2, j].wait_recv()
    stats_on().wait_recv()
    scales = merged()

    @pl.when(half == 0)
    def _():
        for i in range(blocks):
            line = pl.ds(i * size, size)
            part_scale = scales[i * size : (i + 1) * size]
            osend[line] = blend(
                pr[0, line], pr[1, line], part_scale[:, 0:1], part_scale[:, 1:2], reach
            ).astype(jnp.bfloat16)
            o_on(i).start()

    expert_back(0)

    @pl.when(half == 0)
    def _():
        for j in range(1, g):
            unit_copies[1, j].wait_recv()
        for i in range(blocks):
            q = qb[2 * i : 2 * i + 2].reshape(size, 2 * QKD)
            seen = (i + 1) * size
            one, two = weigh(q, seen, True)
            finish(i, blend(one[0], two[0], 1.0 / one[2], lam / two[2], seen))

    expert_back(1)
    back[...] = combine(1, score_m).astype(jnp.bfloat16)
    last = remote(back, back_m, m_send.at[3], m_recv.at[3], mirror, tp)
    last.start()
    sent.append(last)

    @pl.when(half == 1)
    def _():
        for i in range(blocks):
            line = pl.ds(i * size, size)
            seen = (i + 1) * size
            part_scale = scales[i * size : (i + 1) * size]
            mixed = blend(
                pr[0, line, 0:seen],
                pr[1, line, 0:seen],
                part_scale[:, 0:1],
                part_scale[:, 1:2],
                seen,
            )
            o_on(i).wait_recv()
            finish(i, mixed + oret[line].astype(jnp.float32))

    combined = combine(0, score_ref)

    for h in range(heads):

        @pl.when(h != w)
        def _(h=h):
            remote(fin.at[h], att_in.at[h], f_send.at[h], f_recv.at[h], base + h, tp).wait()

        att_ref[:, h * VD : (h + 1) * VD] = att_in[h]

    last.wait_recv()
    out_ref[...] = (combined + back_m[...].astype(jnp.float32)).astype(jnp.bfloat16)

    @pl.when(half == 1)
    def _():
        for s in range(g):
            q_on(s).wait_send()

    @pl.when(half == 0)
    def _():
        for i in range(blocks):
            o_on(i).wait_send()

    stats_on().wait_send()
    for group in (
        tok_copies,
        unit_copies,
        y_copies,
        core_copies,
        more_copies,
        near_copies,
        far_copies,
        back_copies,
    ):
        sent += list(group.values())
    for c in sent:
        c.wait_send()


def local(
    queries,
    key_rows,
    values,
    lambdas,
    head_gain,
    tokens,
    moe_gain,
    routes,
    route_scores,
    w_gate,
    w_up,
    w_down,
):
    n = lax.axis_size("ep")
    heads = lambdas.shape[0]
    rows = queries.shape[0]
    rows_b, model = tokens.shape
    slots = 2 * TOP * rows_b // n
    width = model // 4
    ff = w_gate.shape[2]
    vmem = pl.BlockSpec(memory_space=pltpu.VMEM)
    hbm = pl.BlockSpec(memory_space=pl.ANY)
    smem = pl.BlockSpec(memory_space=pltpu.SMEM)
    bf16, f32 = jnp.bfloat16, jnp.float32
    g = n // 2
    dma = pltpu.SemaphoreType.DMA
    shapes = (
        jax.ShapeDtypeStruct(queries.shape, bf16),
        jax.ShapeDtypeStruct((rows_b, width), bf16),
    )
    inside = (pltpu.VMEM(queries.shape, bf16), pltpu.VMEM((rows_b, width), bf16))
    held = pl.pallas_call(
        functools.partial(step_kernel, n, heads),
        out_shape=inside,
        in_specs=[hbm, hbm, hbm, smem, vmem, hbm] + [vmem] * 3 + [hbm, hbm, hbm],
        out_specs=(vmem, vmem),
        scratch_shapes=[
            pltpu.VMEM((model, ff), bf16),
            pltpu.VMEM((model, ff), bf16),
            pltpu.VMEM((ff, model), bf16),
            pltpu.VMEM((g, rows, VD), bf16),
            pltpu.VMEM((g, rows, VD), bf16),
            pltpu.VMEM((g, rows, VD), bf16),
            pltpu.VMEM((g, rows, VD), bf16),
            pltpu.VMEM((2, g * rows, g * rows), f32),
            pltpu.VMEM((8, g * rows), f32),
            pltpu.VMEM((8, g * rows), f32),
            pltpu.VMEM((g * rows, VD), bf16),
            pltpu.VMEM((g * rows, VD), bf16),
            pltpu.VMEM((g, rows, VD), bf16),
            pltpu.VMEM((heads, rows, VD), bf16),
            pltpu.VMEM((TOP, rows_b), jnp.int32),
            pltpu.VMEM((TOP, rows_b), f32),
            pltpu.VMEM((rows_b, width), bf16),
            pltpu.VMEM((rows_b, width), bf16),
            pltpu.VMEM((2, TOP, rows_b, g * slots), bf16),
            pltpu.VMEM((2, g, slots, width), bf16),
            pltpu.VMEM((4, 2, g, slots, width), bf16),
            pltpu.VMEM((2, 4, g, slots, width), bf16),
            pltpu.VMEM((2, 2, g, slots, width), bf16),
            pltpu.VMEM((2, g, slots, width), bf16),
            pltpu.VMEM((2, g, slots, width), bf16),
            pltpu.VMEM((2, g, slots, width), bf16),
            pltpu.VMEM((2, g, slots, width), bf16),
            pltpu.VMEM((rows_b, width), bf16),
            pltpu.VMEM((rows_b, width), bf16),
            pltpu.VMEM(queries.shape, bf16),
            pltpu.VMEM(queries.shape, bf16),
            pltpu.VMEM(queries.shape, bf16),
            pltpu.VMEM(tokens.shape, bf16),
            dma((7,)),
            dma((4,)),
            dma((4,)),
            dma((2, g)),
            dma((2, g)),
            dma((2, g)),
            dma((2, g)),
            dma((2, 2, g)),
            dma((2, 2, g)),
            dma((3, g)),
            dma((3, g)),
            dma((g,)),
            dma((g,)),
            dma((1 + g // 2,)),
            dma((1 + g // 2,)),
            dma((g,)),
            dma((g,)),
            dma((2, 2)),
            dma((2, 2)),
            dma((2, g)),
            dma((2, g)),
            dma((2, g)),
            dma((2, g)),
        ],
        compiler_params=pltpu.CompilerParams(
            collective_id=0, has_side_effects=True, vmem_limit_bytes=56 * 1024 * 1024
        ),
    )(
        queries,
        key_rows,
        values,
        lambdas,
        head_gain[None, :],
        tokens,
        moe_gain[None, :],
        routes.T,
        route_scores.T,
        w_gate,
        w_up,
        w_down,
    )
    return tuple(held)


def fits(mesh, head_count):
    n, parts = mesh.shape["ep"], mesh.shape["tp"]
    return parts == 4 and n % 2 == 0 and 2 * (head_count // parts) == n


def solution(mesh):
    def step(*args):
        body = local if fits(mesh, args[3].shape[0]) else local_general
        return sharded(mesh, body)(*args)

    return step


def sharded(mesh, body):
    return jax.shard_map(
        body,
        mesh=mesh,
        in_specs=(
            P("ep", "tp"),
            P("ep", "tp"),
            P("ep", "tp"),
            P("tp"),
            P(),
            P("ep", None),
            P(),
            P("ep", None),
            P("ep", None),
            P("ep", None, "tp"),
            P("ep", None, "tp"),
            P("ep", "tp", None),
        ),
        out_specs=(P("ep", "tp"), P("ep", "tp")),
        check_vma=False,
    )
```

```python
import functools

import jax
import jax.numpy as jnp
from jax import lax
from jax.experimental import pallas as pl
from jax.experimental.pallas import tpu as pltpu
from jax.sharding import PartitionSpec as P

QKD = 128
VD = 256
TOP = 2


neg_big = -1e30
head_eps = 1e-05
moe_eps = 1e-06
head_scale = 0.8


def slot_table(routes, experts, capacity):
    flat_routes = routes.reshape(-1)
    onehot = (flat_routes[:, None] == jnp.arange(experts, dtype=jnp.int32)[None, :]).astype(
        jnp.int32
    )
    before = jnp.cumsum(onehot, axis=0) - onehot
    position = jnp.sum(before * onehot, axis=1)
    return (flat_routes * capacity + position).reshape(routes.shape)


def fold_block(state, query_group, query_pos, key_heads, value_heads, key_pos):
    maxima, denominators, accumulated = state
    scores = jnp.einsum(
        "qhmd,khmd->hmqk", query_group, key_heads, preferred_element_type=jnp.float32
    ) * QKD ** (-0.5)
    visible = key_pos[None, :] <= query_pos[:, None]
    scores = jnp.where(visible, scores, neg_big)
    new_max = jnp.maximum(maxima, jnp.max(scores, axis=-1))
    weights = jnp.where(visible, jnp.exp(scores - new_max[..., None]), 0.0)
    accumulated = jnp.einsum(
        "hmqk,khd->hmqd", weights, value_heads, precision=lax.Precision.HIGHEST
    )
    denominators = jnp.sum(weights, axis=-1)
    return (new_max, denominators, accumulated)


def local_general(
    queries,
    key_rows,
    values,
    lambdas,
    head_gain,
    tokens,
    moe_gain,
    routes,
    route_scores,
    w_gate,
    w_up,
    w_down,
):
    rows_a = queries.shape[0]
    half_rows = rows_a // 2
    head_local = lambdas.shape[0]
    ep_count = lax.axis_size("ep")
    ep_index = lax.axis_index("ep")
    early_queries = queries[:half_rows]
    later_queries = queries[half_rows:]
    early_pos = ep_index * rows_a + jnp.arange(half_rows, dtype=jnp.int32)
    later_pos = ep_index * rows_a + half_rows + jnp.arange(half_rows, dtype=jnp.int32)
    query_groups = (
        early_queries.reshape(half_rows, head_local, 2, QKD),
        later_queries.reshape(half_rows, head_local, 2, QKD),
    )
    position_groups = (early_pos, later_pos)
    start_state = (
        jnp.full((head_local, 2, half_rows), neg_big, jnp.float32),
        jnp.zeros((head_local, 2, half_rows), jnp.float32),
        jnp.zeros((head_local, 2, half_rows, VD), jnp.float32),
    )
    totals = (start_state, start_state)
    row_start = jnp.int32(0)
    key_block = lax.all_gather(key_rows, "ep", axis=0, tiled=True)
    value_block = lax.all_gather(values, "ep", axis=0, tiled=True)
    key_count = key_block.shape[0]
    key_heads = key_block.reshape(key_count, head_local, 2, QKD)
    value_heads = value_block.reshape(key_count, head_local, VD).astype(jnp.float32)
    key_pos = jnp.arange(key_count, dtype=jnp.int32)
    updated = []
    for attend_group_index in range(2):
        state = totals[attend_group_index]
        query_group = query_groups[attend_group_index]
        query_pos = position_groups[attend_group_index]
        state = lax.cond(
            row_start <= query_pos[-1],
            lambda held: fold_block(held, query_group, query_pos, key_heads, value_heads, key_pos),
            lambda held: held,
            state,
        )
        updated.append(state)
    folded = (updated[0], updated[1])
    attended_groups = []
    for group_index in range(2):
        maxima, denominators, accumulated = folded[group_index]
        mixed_out = (
            accumulated[:, 0] / denominators[:, 0, :, None]
            - lambdas[:, None, None] * accumulated[:, 1] / denominators[:, 1, :, None]
        )
        scaled = mixed_out * lax.rsqrt(
            jnp.mean(mixed_out * mixed_out, axis=-1, keepdims=True) + head_eps
        )
        scaled = scaled * head_gain * head_scale
        attended_groups.append(
            scaled.transpose(1, 0, 2).reshape(half_rows, head_local * VD).astype(jnp.bfloat16)
        )
    later_out = attended_groups[1]
    attended = jnp.concatenate([attended_groups[0], later_out], axis=0)
    rows_b = tokens.shape[0]
    capacity = 2 * TOP * rows_b // ep_count
    token_f32 = tokens.astype(jnp.float32)
    normed = (
        token_f32
        * lax.rsqrt(jnp.mean(token_f32 * token_f32, axis=-1, keepdims=True) + moe_eps)
        * moe_gain
    ).astype(jnp.bfloat16)
    gate_weights = jax.nn.softmax(route_scores, axis=-1)
    slot_of = slot_table(routes, ep_count, capacity)
    row_ids = jnp.broadcast_to(jnp.arange(rows_b, dtype=jnp.int32)[:, None], slot_of.shape)
    row_of_slot = (
        jnp.zeros((ep_count * capacity,), jnp.int32)
        .at[slot_of.reshape(-1)]
        .set(row_ids.reshape(-1))
    )
    gate_local = w_gate[0]
    up_local = w_up[0]
    down_local = w_down[0]
    outgoing = normed[row_of_slot]
    arrived = lax.all_to_all(outgoing, "ep", split_axis=0, concat_axis=0, tiled=True)
    gate_act = jnp.dot(arrived, gate_local, preferred_element_type=jnp.float32)
    up_act = jnp.dot(arrived, up_local, preferred_element_type=jnp.float32)
    hidden = (jax.nn.silu(gate_act) * up_act).astype(jnp.bfloat16)
    summed = lax.psum_scatter(
        lax.dot_general(
            down_local, hidden, (((0,), (1,)), ((), ())), preferred_element_type=jnp.float32
        ).astype(jnp.bfloat16),
        "tp",
        scatter_dimension=0,
        tiled=True,
    )
    returned = lax.all_to_all(summed, "ep", split_axis=1, concat_axis=1, tiled=True)
    slot_ids = jnp.arange(ep_count * capacity, dtype=jnp.int32)
    combined = jnp.zeros((rows_b, returned.shape[0]), jnp.float32)
    for choice_index in range(TOP):
        picker = (slot_of[:, choice_index, None] == slot_ids[None, :]).astype(jnp.bfloat16)
        picked = lax.dot_general(
            picker, returned, (((1,), (1,)), ((), ())), preferred_element_type=jnp.float32
        )
        combined = combined + gate_weights[:, choice_index, None] * picked
    expert_out = combined.astype(jnp.bfloat16)
    return (attended, expert_out)


MESH = pl.DeviceIdType.MESH


def step_kernel(
    n,
    heads,
    q_in,
    k_in,
    v_in,
    lam_in,
    gain_in,
    tokens_in,
    moe_gain_in,
    routes_in,
    score_in,
    wg_ref,
    wu_ref,
    wd_ref,
    att_ref,
    out_ref,
    wg,
    wu,
    wd,
    qx,
    kk,
    vv,
    qm,
    pr,
    stat_out,
    stat_in,
    osend,
    oret,
    olate,
    fin,
    att_in,
    routes_m,
    score_m,
    dense,
    dense_m,
    pick,
    tok,
    arr,
    part,
    near,
    csum,
    far,
    res,
    ret,
    back,
    back_m,
    q_ref,
    k_ref,
    v_ref,
    tokens_ref,
    lam_ref,
    gain_ref,
    moe_gain_ref,
    routes_ref,
    score_ref,
    w_sem,
    m_send,
    m_recv,
    tok_send,
    tok_recv,
    ty_send,
    ty_recv,
    tc_send,
    tc_recv,
    a_send,
    a_recv,
    kv_send,
    kv_recv,
    qm_send,
    qm_recv,
    st_send,
    st_recv,
    o_send,
    o_recv,
    f_send,
    f_recv,
    rc_send,
    rc_recv,
    ry_send,
    ry_recv,
    e_send,
    e_recv,
):
    me = lax.axis_index("ep")
    tp = lax.axis_index("tp")
    y = tp // 2
    core = tp % 2
    tp_core = y * 2 + 1 - core
    tp_y = (1 - y) * 2 + core
    tp_both = (1 - y) * 2 + 1 - core
    g = n // 2
    half = me // g
    w = me % g
    base = half * g
    mirror = (1 - half) * g + w
    level = me // 2
    x = me % 2
    high = level % 2
    beside = level * 2 + 1 - x
    rows = q_ref.shape[0]
    rows_b = tokens_ref.shape[0]
    slots, width = tok.shape[2:]
    total = g * slots

    def ahead(j):
        return (w, lax.rem(w + g // 2, g), g - 1 - w, w + 1 - 2 * x)[j]

    def remote(src, dst, send, recv, ep, tpi):
        return pltpu.make_async_remote_copy(
            src_ref=src,
            dst_ref=dst,
            send_sem=send,
            recv_sem=recv,
            device_id=(ep, tpi),
            device_id_type=MESH,
        )

    barrier = pltpu.get_barrier_semaphore()
    for j in range(1, g):
        pl.semaphore_signal(barrier, inc=1, device_id=(base + ahead(j), tp), device_id_type=MESH)
    pl.semaphore_signal(barrier, inc=1, device_id=(mirror, tp), device_id_type=MESH)
    hub = g // 2 + x
    crossed = (
        (1, (g + x, g + 1 - x, g + 3 - x)),
        (2, (hub, g // 2 + 1 - x)),
        (3, (g // 2 + 1 - x,)),
    )
    for at, others in crossed:

        @pl.when(level == at)
        def _(others=others):
            for to in others:
                pl.semaphore_signal(barrier, inc=1, device_id=(to, tp), device_id_type=MESH)

    pl.semaphore_signal(barrier, inc=1, device_id=(me, tp_core), device_id_type=MESH)
    pl.semaphore_signal(barrier, inc=1, device_id=(me, tp_y), device_id_type=MESH)
    staged = [
        pltpu.make_async_copy(src, dst, w_sem.at[3 + i])
        for i, (src, dst) in enumerate(
            (
                (tokens_in, tokens_ref),
                (moe_gain_in, moe_gain_ref),
                (routes_in, routes_ref),
                (score_in, score_ref),
                (q_in, q_ref),
                (k_in, k_ref),
                (v_in, v_ref),
                (gain_in, gain_ref),
                (lam_in, lam_ref),
            )
        )
    ]
    for c in staged:
        c.start()
    loads = [
        pltpu.make_async_copy(wg_ref.at[0], wg, w_sem.at[0]),
        pltpu.make_async_copy(wu_ref.at[0], wu, w_sem.at[1]),
        pltpu.make_async_copy(wd_ref.at[0], wd, w_sem.at[2]),
    ]
    for load in loads:
        load.start()

    features = pl.ds(pl.multiple_of(tp * width, width), width)
    for c in staged[:3]:
        c.wait()
    token_f32 = tokens_ref[...].astype(jnp.float32)
    inverse = lax.rsqrt(jnp.mean(token_f32 * token_f32, axis=-1, keepdims=True) + moe_eps)
    dense[...] = (
        tokens_ref[:, features].astype(jnp.float32) * inverse * moe_gain_ref[:, features]
    ).astype(jnp.bfloat16)
    lane = lax.broadcasted_iota(jnp.int32, (rows_b, 128), 1)
    square = (rows_b, rows_b)
    row_at = lax.broadcasted_iota(jnp.int32, square, 0)
    column_at = lax.broadcasted_iota(jnp.int32, square, 1)
    below = jnp.where(column_at < row_at, 1.0, 0.0).astype(jnp.bfloat16)
    slot_ids = lax.broadcasted_iota(jnp.int32, (rows_b, total), 1).astype(jnp.float32)

    def upright(ref, c):
        line = jnp.broadcast_to(ref[c : c + 1, :], square)
        return jnp.sum(
            jnp.where(row_at == column_at, line, jnp.zeros_like(line)), axis=1, keepdims=True
        )

    def choose(group, ref, source):
        named_by = [upright(ref, c) for c in range(TOP)]
        named = [named_by[c] == lane for c in range(TOP)]
        either = jnp.where(named[0] | named[1], 1.0, 0.0).astype(jnp.bfloat16)
        before = jnp.dot(below, either, preferred_element_type=jnp.float32)
        chosen = jnp.zeros((rows_b, total), jnp.float32)
        for c in range(TOP):
            position = jnp.sum(jnp.where(named[c], before, 0.0), axis=1, keepdims=True)
            slot = (named_by[c] - base).astype(jnp.float32) * slots + position
            hit = jnp.where(slot == slot_ids, 1.0, 0.0)
            pick[group, c] = hit.astype(jnp.bfloat16)
            chosen = chosen + hit
        tok[group] = (
            jnp.dot(
                chosen.T.astype(jnp.bfloat16), source[...], preferred_element_type=jnp.float32
            )
            .astype(jnp.bfloat16)
            .reshape(g, slots, width)
        )

    choose(0, routes_ref, dense)
    pl.semaphore_wait(barrier, g + 2 + lax.rem(4 - level, 4))
    for c in staged[3:]:
        c.wait()
    sent = []
    mirrored = [
        remote(routes_ref, routes_m, m_send.at[0], m_recv.at[0], mirror, tp),
        remote(score_ref, score_m, m_send.at[1], m_recv.at[1], mirror, tp),
        remote(dense, dense_m, m_send.at[2], m_recv.at[2], mirror, tp),
    ]
    for c in mirrored:
        c.start()
    sent += mirrored
    tok_copies = {}

    def scatter(group):
        for j in range(1, g):
            d = ahead(j)
            c = remote(
                tok.at[group, d],
                arr.at[tp, group, w],
                tok_send.at[group, j],
                tok_recv.at[group, j],
                base + d,
                tp,
            )
            c.start()
            tok_copies[group, j] = c

    def pair(which):
        return pl.ds(pl.multiple_of(which * 2 * VD, 2 * VD), 2 * VD)

    def unit(which):
        src, dst = ((k_ref, kk.at[2 + x]), (q_ref, qx.at[x]), (v_ref, vv.at[2 + x]))[which]
        return remote(
            src.at[:, pair(1 - x)], dst, a_send.at[which], a_recv.at[which], beside, tp
        )

    def own_up(which):
        src, dst = ((k_ref, kk), (v_ref, vv))[which]
        return remote(
            src.at[:, pair(x)],
            dst.at[x],
            kv_send.at[which, x],
            kv_recv.at[which, x],
            me + 2,
            tp,
        )

    def other_up(which):
        buf = (kk, vv)[which]
        return remote(
            buf.at[3 - x],
            buf.at[1 - x],
            kv_send.at[which, 1 - x],
            kv_recv.at[which, 1 - x],
            me + 2,
            tp,
        )

    def from_below(which, b):
        buf = (kk, vv)[which]
        return remote(
            buf.at[b], buf.at[b], kv_send.at[which, b], kv_recv.at[which, b], me - 2, tp
        )

    def own_q():
        return remote(
            q_ref.at[:, pair(x)],
            qm.at[high, x],
            qm_send.at[high, x],
            qm_recv.at[high, x],
            hub,
            tp,
        )

    def other_q():
        return remote(
            qx.at[1 - x],
            qm.at[high, 1 - x],
            qm_send.at[high, 1 - x],
            qm_recv.at[high, 1 - x],
            hub,
            tp,
        )

    def q_came(late, b):
        return remote(
            qm.at[late, b],
            qm.at[late, b],
            qm_send.at[late, b],
            qm_recv.at[late, b],
            g + 2 * late + x,
            tp,
        )

    y_copies, core_copies, more_copies = {}, {}, {}

    def hand(group, j):
        s = ahead(j)
        if j == 0:
            src = tok.at[group, w]
            arr[tp, group, w] = tok[group, w]
        else:
            tok_copies[group, j].wait_recv()
            src = arr.at[tp, group, s]
        c = remote(
            src, arr.at[tp, group, s], ty_send.at[group, j], ty_recv.at[group, j], me, tp_y
        )
        c.start()
        y_copies[group, j] = c
        c = remote(
            src,
            arr.at[tp, group, s],
            tc_send.at[0, group, j],
            tc_recv.at[0, group, j],
            me,
            tp_core,
        )
        c.start()
        core_copies[group, j] = c

    scatter(0)

    @pl.when(half == 1)
    def _():
        unit(1).start()

    unit(0).start()
    hand(0, 0)
    kk[2 + x] = k_ref[:, pair(x)]
    qx[x] = q_ref[:, pair(x)]
    vv[2 + x] = v_ref[:, pair(x)]
    for j in (3, 1, 2):
        hand(0, j)
    for c in mirrored:
        c.wait_recv()
    choose(1, routes_m, dense_m)
    scatter(1)
    hand(1, 0)
    unit(2).start()

    @pl.when(half == 0)
    def _():
        unit(1).start()

    @pl.when(half == 1)
    def _():
        own_q().start()
        unit(1).wait_recv()
        other_q().start()

    @pl.when(high == 0)
    def _():
        own_up(0).start()
        unit(0).wait_recv()
        other_up(0).start()
        own_up(1).start()

    def first_products(group, quarter):
        a = arr[quarter, group].reshape(total, width)
        deep = pl.ds(pl.multiple_of(quarter * width, width), width)
        return (
            jnp.dot(a, wg[deep, :], preferred_element_type=jnp.float32),
            jnp.dot(a, wu[deep, :], preferred_element_type=jnp.float32),
        )

    def near_half(group):
        one = first_products(group, tp)
        for j in range(g):
            core_copies[group, j].wait_recv()
        two = first_products(group, tp_core)
        return one[0] + two[0], one[1] + two[1]

    order = (tp_both, tp_y, tp_core, tp)
    near_copies, far_copies = {}, {}

    def far_half(group, gate, up):
        for j in (0, 3, 1, 2):
            s = ahead(j)
            y_copies[group, j].wait_recv()
            c = remote(
                arr.at[tp_y, group, s],
                arr.at[tp_y, group, s],
                tc_send.at[1, group, j],
                tc_recv.at[1, group, j],
                me,
                tp_core,
            )
            c.start()
            more_copies[group, j] = c
        more = first_products(group, tp_y)
        gate, up = gate + more[0], up + more[1]
        for j in range(g):
            more_copies[group, j].wait_recv()
        more = first_products(group, tp_both)
        gate, up = gate + more[0], up + more[1]
        return (jax.nn.silu(gate) * up).astype(jnp.bfloat16)

    def second_products(group, hidden):
        for i in range(4):
            cols = pl.ds(pl.multiple_of(order[i] * width, width), width)
            part[group, i] = (
                jnp.dot(hidden, wd[:, cols], preferred_element_type=jnp.float32)
                .astype(jnp.bfloat16)
                .reshape(g, slots, width)
            )
            if i % 2 == 0:
                h = i // 2
                c = remote(
                    part.at[group, i],
                    near.at[group, h],
                    rc_send.at[group, h],
                    rc_recv.at[group, h],
                    me,
                    tp_core,
                )
                c.start()
                near_copies[group, h] = c
        near_copies[group, 0].wait_recv()
        for j in [*range(1, g), 0]:
            d = ahead(j)
            csum[group, d] = (
                part[group, 1, d].astype(jnp.float32) + near[group, 0, d].astype(jnp.float32)
            ).astype(jnp.bfloat16)
            c = remote(
                csum.at[group, d],
                far.at[group, d],
                ry_send.at[group, j],
                ry_recv.at[group, j],
                me,
                tp_y,
            )
            c.start()
            far_copies[group, j] = c

    back_copies = {}

    def expert_back(group):
        near_copies[group, 1].wait_recv()
        for j in [*range(1, g), 0]:
            d = ahead(j)
            far_copies[group, j].wait_recv()
            val = (
                part[group, 3, d].astype(jnp.float32)
                + near[group, 1, d].astype(jnp.float32)
                + far[group, d].astype(jnp.float32)
            ).astype(jnp.bfloat16)
            if j == 0:
                ret[group, w] = val
            else:
                res[group, d] = val
                c = remote(
                    res.at[group, d],
                    ret.at[group, w],
                    e_send.at[group, j],
                    e_recv.at[group, j],
                    base + d,
                    tp,
                )
                c.start()
                back_copies[group, j] = c

    def combine(group, ref):
        for j in range(1, g):
            back_copies[group, j].wait_recv()
        first, second = upright(ref, 0), upright(ref, 1)
        top = jnp.maximum(first, second)
        raised = (jnp.exp(first - top), jnp.exp(second - top))
        returned = ret[group].reshape(total, width)
        combined = jnp.zeros(out_ref.shape, jnp.float32)
        for c in range(TOP):
            picked = jnp.dot(pick[group, c], returned, preferred_element_type=jnp.float32)
            combined = combined + raised[c] / (raised[0] + raised[1]) * picked
        return combined

    lam = [lam_ref[x * 2 + h] for h in range(2)]
    size = 2 * rows
    diag = (
        lax.broadcasted_iota(jnp.int32, (size, size), 1)
        <= lax.broadcasted_iota(jnp.int32, (size, size), 0)
    )
    stat_lane = lax.broadcasted_iota(jnp.int32, (size, 128), 1)

    def columns(h, m):
        return slice(h * VD + m * QKD, h * VD + (m + 1) * QKD)

    def weigh(q, first, h, masked):
        found = []
        seen = (4 - first) * rows
        for m in range(2):
            k = kk[first:4].reshape(seen, 2 * VD)[:, columns(h, m)]
            scores = lax.dot_general(
                q[:, columns(h, m)],
                k,
                (((1,), (1,)), ((), ())),
                preferred_element_type=jnp.float32,
            ) * QKD ** (-0.5)
            if masked:
                last = jnp.where(diag, scores[:, seen - size :], neg_big)
                scores = (
                    last
                    if seen == size
                    else jnp.concatenate([scores[:, : seen - size], last], axis=1)
                )
            top = jnp.max(scores, axis=-1, keepdims=True)
            weights = jnp.exp(scores - top)
            found.append((weights, top, jnp.sum(weights, axis=-1, keepdims=True)))
        return found

    def blend(one, two, scale_one, scale_two, first, h):
        v = vv[first:4].reshape((4 - first) * rows, 2 * VD)[:, h * VD : (h + 1) * VD]
        mixed = (one * scale_one - two * scale_two).astype(jnp.bfloat16)
        return jnp.dot(mixed, v, preferred_element_type=jnp.float32)

    def keep(late, place, q, first, masked):
        seen = (4 - first) * rows
        packed = jnp.zeros((size, 128), jnp.float32)
        for h in range(2):
            for m, (weights, top, bottom) in enumerate(weigh(q, first, h, masked)):
                pr[place, h, m, :, 0:seen] = weights
                packed = jnp.where(stat_lane == 4 * h + 2 * m, top, packed)
                packed = jnp.where(stat_lane == 4 * h + 2 * m + 1, bottom, packed)
        stat_out[late] = packed.T[0:8]

    def stats_on(late, to):
        return remote(
            stat_out.at[late], stat_in.at[late], st_send.at[late], st_recv.at[late], to, tp
        )

    def merged(late):
        mine, other = stat_out[late], stat_in[late]
        at = lax.broadcasted_iota(jnp.int32, (128, size), 0)
        table = jnp.zeros((128, size), jnp.float32)
        for h in range(2):
            for m in range(2):
                r = 4 * h + 2 * m
                top, bottom = mine[r : r + 1], mine[r + 1 : r + 2]
                top_o, bottom_o = other[r : r + 1], other[r + 1 : r + 2]
                high_top = jnp.maximum(top, top_o)
                share = jnp.exp(top - high_top)
                scale = share / (bottom * share + bottom_o * jnp.exp(top_o - high_top))
                if m == 1:
                    scale = scale * lam[h]
                table = jnp.where(at == 2 * h + m, scale, table)
        return table.T

    def o_on(late, h, b):
        return remote(
            osend.at[late, h, b],
            oret.at[x, h],
            o_send.at[late, h, b],
            o_recv.at[x, h],
            g + 2 * late + b,
            tp,
        )

    def o_came(side, h):
        return remote(
            oret.at[side, h],
            oret.at[side, h],
            o_send.at[0, h, 0],
            o_recv.at[side, h],
            g // 2 + side,
            tp,
        )

    def f_on(h):
        return remote(fin.at[h, 1 - x], att_in.at[h], f_send.at[h], f_recv.at[h], beside, tp)

    def normal(mixed):
        scaled = mixed * lax.rsqrt(jnp.mean(mixed * mixed, axis=-1, keepdims=True) + head_eps)
        return (scaled * gain_ref[...] * head_scale).astype(jnp.bfloat16)

    def finish(h, mixed):
        fin[h] = normal(mixed).reshape(2, rows, VD)
        f_on(h).start()

    def own_rows():
        return qx[...].reshape(size, 2 * VD)

    def below_came(which):
        for b in range(2):
            from_below(which, b).wait_recv()

    def settle(first):
        for h in range(2):
            one, two = weigh(own_rows(), first, h, True)
            finish(h, blend(one[0], two[0], 1.0 / one[2], lam[h] / two[2], first, h))

    def late_scores(late):
        for b in range(2):
            q_came(late, b).wait_recv()
        keep(late, late, qm[late].reshape(size, 2 * VD), 0, False)
        stats_on(late, g + 2 * late + x).start()

    def late_out(late):
        stats_on(late, g + 2 * late + x).wait_recv()
        scales = merged(late)
        for h in range(2):
            o = blend(
                pr[late, h, 0],
                pr[late, h, 1],
                scales[:, 2 * h : 2 * h + 1],
                scales[:, 2 * h + 1 : 2 * h + 2],
                0,
                h,
            )
            osend[late, h] = o.astype(jnp.bfloat16).reshape(2, rows, VD)
            for b in range(2):
                o_on(late, h, b).start()

    def own_late(late, first):
        seen = (4 - first) * rows
        stats_on(late, hub).wait_recv()
        scales = merged(late)
        for h in range(2):
            o = blend(
                pr[0, h, 0, :, 0:seen],
                pr[0, h, 1, :, 0:seen],
                scales[:, 2 * h : 2 * h + 1],
                scales[:, 2 * h + 1 : 2 * h + 2],
                first,
                h,
            ).reshape(2, rows, VD)
            olate[h] = o
            fin[h] = o.astype(jnp.bfloat16)
            f_on(h).start()

    at_level = [level == i for i in range(4)]

    loads[0].wait()
    loads[1].wait()
    gate, up = near_half(0)
    hidden = far_half(0, gate, up)
    for j in (3, 1, 2):
        hand(1, j)
    loads[2].wait()
    second_products(0, hidden)

    @pl.when(at_level[2])
    def _():
        keep(0, 0, own_rows(), 2, True)
        stats_on(0, hub).start()

    @pl.when(at_level[3])
    def _():
        unit(0).wait_recv()
        below_came(0)
        keep(1, 0, own_rows(), 0, True)
        stats_on(1, hub).start()

    gate, up = near_half(1)

    @pl.when(high == 0)
    def _():
        unit(2).wait_recv()
        other_up(1).start()

    @pl.when(at_level[1])
    def _():
        unit(0).wait_recv()
        below_came(0)
        late_scores(0)

    hidden = far_half(1, gate, up)
    second_products(1, hidden)

    @pl.when(at_level[1])
    def _():
        late_scores(1)
        unit(2).wait_recv()
        below_came(1)
        late_out(0)
        late_out(1)

    expert_back(0)

    @pl.when(at_level[0])
    def _():
        unit(1).wait_recv()
        settle(2)

    @pl.when(at_level[2])
    def _():
        own_late(0, 2)

    @pl.when(at_level[3])
    def _():
        unit(2).wait_recv()
        below_came(1)
        own_late(1, 0)

    expert_back(1)

    @pl.when(at_level[1])
    def _():
        unit(1).wait_recv()
        settle(0)

    back[...] = combine(1, score_m).astype(jnp.bfloat16)
    last = remote(back, back_m, m_send.at[3], m_recv.at[3], mirror, tp)
    last.start()
    sent.append(last)
    combined = combine(0, score_ref)

    def head_columns(side, h):
        return pl.ds(pl.multiple_of((2 * side + h) * VD, VD), VD)

    @pl.when(half == 1)
    def _():
        for h in range(2):
            o_came(x, h).wait_recv()
            att_ref[:, head_columns(x, h)] = normal(
                olate[h, x] + oret[x, h].astype(jnp.float32)
            )
        for h in range(2):
            f_on(h).wait()
            o_came(1 - x, h).wait_recv()
            att_ref[:, head_columns(1 - x, h)] = normal(
                att_in[h].astype(jnp.float32) + oret[1 - x, h].astype(jnp.float32)
            )

    @pl.when(half == 0)
    def _():
        for h in range(2):
            att_ref[:, head_columns(x, h)] = fin[h, x]
        for h in range(2):
            f_on(h).wait()
            att_ref[:, head_columns(1 - x, h)] = att_in[h]

    last.wait_recv()
    out_ref[...] = (combined + back_m[...].astype(jnp.float32)).astype(jnp.bfloat16)

    @pl.when(half == 1)
    def _():
        own_q().wait_send()
        other_q().wait_send()
        stats_on(high, hub).wait_send()

    @pl.when(high == 0)
    def _():
        for which in range(2):
            own_up(which).wait_send()
            other_up(which).wait_send()

    @pl.when(at_level[1])
    def _():
        for late in range(2):
            stats_on(late, g + 2 * late + x).wait_send()
            for h in range(2):
                for b in range(2):
                    o_on(late, h, b).wait_send()

    for group in (
        tok_copies,
        y_copies,
        core_copies,
        more_copies,
        near_copies,
        far_copies,
        back_copies,
    ):
        sent += list(group.values())
    for c in sent:
        c.wait_send()
    for which in range(3):
        unit(which).wait_send()


def local(
    queries,
    key_rows,
    values,
    lambdas,
    head_gain,
    tokens,
    moe_gain,
    routes,
    route_scores,
    w_gate,
    w_up,
    w_down,
):
    n = lax.axis_size("ep")
    heads = lambdas.shape[0]
    rows = queries.shape[0]
    rows_b, model = tokens.shape
    slots = 2 * TOP * rows_b // n
    width = model // 4
    ff = w_gate.shape[2]
    vmem = pl.BlockSpec(memory_space=pltpu.VMEM)
    hbm = pl.BlockSpec(memory_space=pl.ANY)
    bf16, f32 = jnp.bfloat16, jnp.float32
    g = n // 2
    dma = pltpu.SemaphoreType.DMA
    shapes = (
        jax.ShapeDtypeStruct(queries.shape, bf16),
        jax.ShapeDtypeStruct((rows_b, width), bf16),
    )
    inside = (pltpu.VMEM(queries.shape, bf16), pltpu.VMEM((rows_b, width), bf16))
    held = pl.pallas_call(
        functools.partial(step_kernel, n, heads),
        out_shape=inside,
        in_specs=[hbm] * 12,
        out_specs=(vmem, vmem),
        scratch_shapes=[
            pltpu.VMEM((model, ff), bf16),
            pltpu.VMEM((model, ff), bf16),
            pltpu.VMEM((ff, model), bf16),
            pltpu.VMEM((2, rows, 2 * VD), bf16),
            pltpu.VMEM((4, rows, 2 * VD), bf16),
            pltpu.VMEM((4, rows, 2 * VD), bf16),
            pltpu.VMEM((2, 2, rows, 2 * VD), bf16),
            pltpu.VMEM((2, 2, 2, 2 * rows, 4 * rows), f32),
            pltpu.VMEM((2, 8, 2 * rows), f32),
            pltpu.VMEM((2, 8, 2 * rows), f32),
            pltpu.VMEM((2, 2, 2, rows, VD), bf16),
            pltpu.VMEM((2, 2, rows, VD), bf16),
            pltpu.VMEM((2, 2, rows, VD), f32),
            pltpu.VMEM((2, 2, rows, VD), bf16),
            pltpu.VMEM((2, rows, VD), bf16),
            pltpu.VMEM((TOP, rows_b), jnp.int32),
            pltpu.VMEM((TOP, rows_b), f32),
            pltpu.VMEM((rows_b, width), bf16),
            pltpu.VMEM((rows_b, width), bf16),
            pltpu.VMEM((2, TOP, rows_b, g * slots), bf16),
            pltpu.VMEM((2, g, slots, width), bf16),
            pltpu.VMEM((4, 2, g, slots, width), bf16),
            pltpu.VMEM((2, 4, g, slots, width), bf16),
            pltpu.VMEM((2, 2, g, slots, width), bf16),
            pltpu.VMEM((2, g, slots, width), bf16),
            pltpu.VMEM((2, g, slots, width), bf16),
            pltpu.VMEM((2, g, slots, width), bf16),
            pltpu.VMEM((2, g, slots, width), bf16),
            pltpu.VMEM((rows_b, width), bf16),
            pltpu.VMEM((rows_b, width), bf16),
            pltpu.VMEM(queries.shape, bf16),
            pltpu.VMEM(queries.shape, bf16),
            pltpu.VMEM(queries.shape, bf16),
            pltpu.VMEM(tokens.shape, bf16),
            pltpu.SMEM(lambdas.shape, f32),
            pltpu.VMEM((1, VD), f32),
            pltpu.VMEM((1, model), f32),
            pltpu.VMEM((TOP, rows_b), jnp.int32),
            pltpu.VMEM((TOP, rows_b), f32),
            dma((12,)),
            dma((4,)),
            dma((4,)),
            dma((2, g)),
            dma((2, g)),
            dma((2, g)),
            dma((2, g)),
            dma((2, 2, g)),
            dma((2, 2, g)),
            dma((3,)),
            dma((3,)),
            dma((2, 2)),
            dma((2, 2)),
            dma((2, 2)),
            dma((2, 2)),
            dma((2,)),
            dma((2,)),
            dma((2, 2, 2)),
            dma((2, 2)),
            dma((2,)),
            dma((2,)),
            dma((2, 2)),
            dma((2, 2)),
            dma((2, g)),
            dma((2, g)),
            dma((2, g)),
            dma((2, g)),
        ],
        compiler_params=pltpu.CompilerParams(
            collective_id=0, has_side_effects=True, vmem_limit_bytes=56 * 1024 * 1024
        ),
    )(
        queries,
        key_rows,
        values,
        lambdas,
        head_gain[None, :],
        tokens,
        moe_gain[None, :],
        routes.T,
        route_scores.T,
        w_gate,
        w_up,
        w_down,
    )
    return tuple(held)


def fits(mesh, head_count):
    n, parts = mesh.shape["ep"], mesh.shape["tp"]
    return parts == 4 and n == 2 * parts and head_count == parts * parts


def solution(mesh):
    def step(*args):
        body = local if fits(mesh, args[3].shape[0]) else local_general
        return sharded(mesh, body)(*args)

    return step


def sharded(mesh, body):
    return jax.shard_map(
        body,
        mesh=mesh,
        in_specs=(
            P("ep", "tp"),
            P("ep", "tp"),
            P("ep", "tp"),
            P("tp"),
            P(),
            P("ep", None),
            P(),
            P("ep", None),
            P("ep", None),
            P("ep", None, "tp"),
            P("ep", None, "tp"),
            P("ep", "tp", None),
        ),
        out_specs=(P("ep", "tp"), P("ep", "tp")),
        check_vma=False,
    )
```

```python
import functools

import jax
import jax.numpy as jnp
from jax import lax
from jax.experimental import pallas as pl
from jax.experimental.pallas import tpu as pltpu
from jax.sharding import PartitionSpec as P

QKD = 128
VD = 256
TOP = 2


neg_big = -1e30
head_eps = 1e-05
moe_eps = 1e-06
head_scale = 0.8


def slot_table(routes, experts, capacity):
    flat_routes = routes.reshape(-1)
    onehot = (flat_routes[:, None] == jnp.arange(experts, dtype=jnp.int32)[None, :]).astype(
        jnp.int32
    )
    before = jnp.cumsum(onehot, axis=0) - onehot
    position = jnp.sum(before * onehot, axis=1)
    return (flat_routes * capacity + position).reshape(routes.shape)


def fold_block(state, query_group, query_pos, key_heads, value_heads, key_pos):
    maxima, denominators, accumulated = state
    scores = jnp.einsum(
        "qhmd,khmd->hmqk", query_group, key_heads, preferred_element_type=jnp.float32
    ) * QKD ** (-0.5)
    visible = key_pos[None, :] <= query_pos[:, None]
    scores = jnp.where(visible, scores, neg_big)
    new_max = jnp.maximum(maxima, jnp.max(scores, axis=-1))
    weights = jnp.where(visible, jnp.exp(scores - new_max[..., None]), 0.0)
    accumulated = jnp.einsum(
        "hmqk,khd->hmqd", weights, value_heads, precision=lax.Precision.HIGHEST
    )
    denominators = jnp.sum(weights, axis=-1)
    return (new_max, denominators, accumulated)


def local_general(
    queries,
    key_rows,
    values,
    lambdas,
    head_gain,
    tokens,
    moe_gain,
    routes,
    route_scores,
    w_gate,
    w_up,
    w_down,
):
    rows_a = queries.shape[0]
    half_rows = rows_a // 2
    head_local = lambdas.shape[0]
    ep_count = lax.axis_size("ep")
    ep_index = lax.axis_index("ep")
    early_queries = queries[:half_rows]
    later_queries = queries[half_rows:]
    early_pos = ep_index * rows_a + jnp.arange(half_rows, dtype=jnp.int32)
    later_pos = ep_index * rows_a + half_rows + jnp.arange(half_rows, dtype=jnp.int32)
    query_groups = (
        early_queries.reshape(half_rows, head_local, 2, QKD),
        later_queries.reshape(half_rows, head_local, 2, QKD),
    )
    position_groups = (early_pos, later_pos)
    start_state = (
        jnp.full((head_local, 2, half_rows), neg_big, jnp.float32),
        jnp.zeros((head_local, 2, half_rows), jnp.float32),
        jnp.zeros((head_local, 2, half_rows, VD), jnp.float32),
    )
    totals = (start_state, start_state)
    row_start = jnp.int32(0)
    key_block = lax.all_gather(key_rows, "ep", axis=0, tiled=True)
    value_block = lax.all_gather(values, "ep", axis=0, tiled=True)
    key_count = key_block.shape[0]
    key_heads = key_block.reshape(key_count, head_local, 2, QKD)
    value_heads = value_block.reshape(key_count, head_local, VD).astype(jnp.float32)
    key_pos = jnp.arange(key_count, dtype=jnp.int32)
    updated = []
    for attend_group_index in range(2):
        state = totals[attend_group_index]
        query_group = query_groups[attend_group_index]
        query_pos = position_groups[attend_group_index]
        state = lax.cond(
            row_start <= query_pos[-1],
            lambda held: fold_block(held, query_group, query_pos, key_heads, value_heads, key_pos),
            lambda held: held,
            state,
        )
        updated.append(state)
    folded = (updated[0], updated[1])
    attended_groups = []
    for group_index in range(2):
        maxima, denominators, accumulated = folded[group_index]
        mixed_out = (
            accumulated[:, 0] / denominators[:, 0, :, None]
            - lambdas[:, None, None] * accumulated[:, 1] / denominators[:, 1, :, None]
        )
        scaled = mixed_out * lax.rsqrt(
            jnp.mean(mixed_out * mixed_out, axis=-1, keepdims=True) + head_eps
        )
        scaled = scaled * head_gain * head_scale
        attended_groups.append(
            scaled.transpose(1, 0, 2).reshape(half_rows, head_local * VD).astype(jnp.bfloat16)
        )
    later_out = attended_groups[1]
    attended = jnp.concatenate([attended_groups[0], later_out], axis=0)
    rows_b = tokens.shape[0]
    capacity = 2 * TOP * rows_b // ep_count
    token_f32 = tokens.astype(jnp.float32)
    normed = (
        token_f32
        * lax.rsqrt(jnp.mean(token_f32 * token_f32, axis=-1, keepdims=True) + moe_eps)
        * moe_gain
    ).astype(jnp.bfloat16)
    gate_weights = jax.nn.softmax(route_scores, axis=-1)
    slot_of = slot_table(routes, ep_count, capacity)
    row_ids = jnp.broadcast_to(jnp.arange(rows_b, dtype=jnp.int32)[:, None], slot_of.shape)
    row_of_slot = (
        jnp.zeros((ep_count * capacity,), jnp.int32)
        .at[slot_of.reshape(-1)]
        .set(row_ids.reshape(-1))
    )
    gate_local = w_gate[0]
    up_local = w_up[0]
    down_local = w_down[0]
    outgoing = normed[row_of_slot]
    arrived = lax.all_to_all(outgoing, "ep", split_axis=0, concat_axis=0, tiled=True)
    gate_act = jnp.dot(arrived, gate_local, preferred_element_type=jnp.float32)
    up_act = jnp.dot(arrived, up_local, preferred_element_type=jnp.float32)
    hidden = (jax.nn.silu(gate_act) * up_act).astype(jnp.bfloat16)
    summed = lax.psum_scatter(
        lax.dot_general(
            down_local, hidden, (((0,), (1,)), ((), ())), preferred_element_type=jnp.float32
        ).astype(jnp.bfloat16),
        "tp",
        scatter_dimension=0,
        tiled=True,
    )
    returned = lax.all_to_all(summed, "ep", split_axis=1, concat_axis=1, tiled=True)
    slot_ids = jnp.arange(ep_count * capacity, dtype=jnp.int32)
    combined = jnp.zeros((rows_b, returned.shape[0]), jnp.float32)
    for choice_index in range(TOP):
        picker = (slot_of[:, choice_index, None] == slot_ids[None, :]).astype(jnp.bfloat16)
        picked = lax.dot_general(
            picker, returned, (((1,), (1,)), ((), ())), preferred_element_type=jnp.float32
        )
        combined = combined + gate_weights[:, choice_index, None] * picked
    expert_out = combined.astype(jnp.bfloat16)
    return (attended, expert_out)


MESH = pl.DeviceIdType.MESH


def step_kernel(
    n,
    heads,
    q_in,
    k_in,
    v_in,
    lam_in,
    gain_in,
    tokens_in,
    moe_gain_in,
    routes_in,
    score_in,
    wg_ref,
    wu_ref,
    wd_ref,
    att_ref,
    out_ref,
    wg,
    wu,
    wd,
    qx,
    kk,
    vv,
    qm,
    pr,
    stat_out,
    stat_in,
    osend,
    oret,
    olate,
    fin,
    att_in,
    routes_m,
    score_m,
    dense,
    dense_m,
    pick,
    tok,
    arr,
    part,
    near,
    csum,
    far,
    res,
    ret,
    back,
    back_m,
    q_ref,
    k_ref,
    v_ref,
    tokens_ref,
    lam_ref,
    gain_ref,
    moe_gain_ref,
    routes_ref,
    score_ref,
    w_sem,
    m_send,
    m_recv,
    tok_send,
    tok_recv,
    ty_send,
    ty_recv,
    tc_send,
    tc_recv,
    a_send,
    a_recv,
    kv_send,
    kv_recv,
    qm_send,
    qm_recv,
    st_send,
    st_recv,
    o_send,
    o_recv,
    f_send,
    f_recv,
    rc_send,
    rc_recv,
    ry_send,
    ry_recv,
    e_send,
    e_recv,
):
    me = lax.axis_index("ep")
    tp = lax.axis_index("tp")
    y = tp // 2
    core = tp % 2
    tp_core = y * 2 + 1 - core
    tp_y = (1 - y) * 2 + core
    tp_both = (1 - y) * 2 + 1 - core
    g = n // 2
    half = me // g
    w = me % g
    base = half * g
    mirror = (1 - half) * g + w
    level = me // 2
    x = me % 2
    high = level % 2
    beside = level * 2 + 1 - x
    rows = q_ref.shape[0]
    rows_b = tokens_ref.shape[0]
    slots, width = tok.shape[2:]
    total = g * slots

    def ahead(j):
        return (w, lax.rem(w + g // 2, g), g - 1 - w, w + 1 - 2 * x)[j]

    def remote(src, dst, send, recv, ep, tpi):
        return pltpu.make_async_remote_copy(
            src_ref=src,
            dst_ref=dst,
            send_sem=send,
            recv_sem=recv,
            device_id=(ep, tpi),
            device_id_type=MESH,
        )

    barrier = pltpu.get_barrier_semaphore()
    for j in range(1, g):
        pl.semaphore_signal(barrier, inc=1, device_id=(base + ahead(j), tp), device_id_type=MESH)
    pl.semaphore_signal(barrier, inc=1, device_id=(mirror, tp), device_id_type=MESH)
    hub = g // 2 + x
    crossed = (
        (1, (g + x, g + 1 - x, g + 3 - x)),
        (2, (hub, g // 2 + 1 - x)),
        (3, (g // 2 + 1 - x,)),
    )
    for at, others in crossed:

        @pl.when(level == at)
        def _(others=others):
            for to in others:
                pl.semaphore_signal(barrier, inc=1, device_id=(to, tp), device_id_type=MESH)

    pl.semaphore_signal(barrier, inc=1, device_id=(me, tp_core), device_id_type=MESH)
    pl.semaphore_signal(barrier, inc=1, device_id=(me, tp_y), device_id_type=MESH)
    staged = [
        pltpu.make_async_copy(src, dst, w_sem.at[3 + i])
        for i, (src, dst) in enumerate(
            (
                (tokens_in, tokens_ref),
                (moe_gain_in, moe_gain_ref),
                (routes_in, routes_ref),
                (score_in, score_ref),
                (q_in, q_ref),
                (k_in, k_ref),
                (v_in, v_ref),
                (gain_in, gain_ref),
                (lam_in, lam_ref),
            )
        )
    ]
    for c in staged:
        c.start()
    loads = [
        pltpu.make_async_copy(wg_ref.at[0], wg, w_sem.at[0]),
        pltpu.make_async_copy(wu_ref.at[0], wu, w_sem.at[1]),
        pltpu.make_async_copy(wd_ref.at[0], wd, w_sem.at[2]),
    ]
    for load in loads:
        load.start()

    features = pl.ds(pl.multiple_of(tp * width, width), width)
    for c in staged[:3]:
        c.wait()
    token_f32 = tokens_ref[...].astype(jnp.float32)
    inverse = lax.rsqrt(jnp.mean(token_f32 * token_f32, axis=-1, keepdims=True) + moe_eps)
    dense[...] = (
        tokens_ref[:, features].astype(jnp.float32) * inverse * moe_gain_ref[:, features]
    ).astype(jnp.bfloat16)
    lane = lax.broadcasted_iota(jnp.int32, (rows_b, 128), 1)
    square = (rows_b, rows_b)
    row_at = lax.broadcasted_iota(jnp.int32, square, 0)
    column_at = lax.broadcasted_iota(jnp.int32, square, 1)
    below = jnp.where(column_at < row_at, 1.0, 0.0).astype(jnp.bfloat16)
    slot_ids = lax.broadcasted_iota(jnp.int32, (rows_b, total), 1).astype(jnp.float32)

    def upright(ref, c):
        line = jnp.broadcast_to(ref[c : c + 1, :], square)
        return jnp.sum(
            jnp.where(row_at == column_at, line, jnp.zeros_like(line)), axis=1, keepdims=True
        )

    def choose(group, ref, source):
        named_by = [upright(ref, c) for c in range(TOP)]
        named = [named_by[c] == lane for c in range(TOP)]
        either = jnp.where(named[0] | named[1], 1.0, 0.0).astype(jnp.bfloat16)
        before = jnp.dot(below, either, preferred_element_type=jnp.float32)
        chosen = jnp.zeros((rows_b, total), jnp.float32)
        for c in range(TOP):
            position = jnp.sum(jnp.where(named[c], before, 0.0), axis=1, keepdims=True)
            slot = (named_by[c] - base).astype(jnp.float32) * slots + position
            hit = jnp.where(slot == slot_ids, 1.0, 0.0)
            pick[group, c] = hit.astype(jnp.bfloat16)
            chosen = chosen + hit
        tok[group] = (
            jnp.dot(
                chosen.T.astype(jnp.bfloat16), source[...], preferred_element_type=jnp.float32
            )
            .astype(jnp.bfloat16)
            .reshape(g, slots, width)
        )

    choose(0, routes_ref, dense)
    pl.semaphore_wait(barrier, g + 2 + lax.rem(4 - level, 4))
    for c in staged[3:]:
        c.wait()
    sent = []
    mirrored = [
        remote(routes_ref, routes_m, m_send.at[0], m_recv.at[0], mirror, tp),
        remote(score_ref, score_m, m_send.at[1], m_recv.at[1], mirror, tp),
        remote(dense, dense_m, m_send.at[2], m_recv.at[2], mirror, tp),
    ]
    for c in mirrored:
        c.start()
    sent += mirrored
    tok_copies = {}

    def scatter(group):
        for j in range(1, g):
            d = ahead(j)
            c = remote(
                tok.at[group, d],
                arr.at[tp, group, w],
                tok_send.at[group, j],
                tok_recv.at[group, j],
                base + d,
                tp,
            )
            c.start()
            tok_copies[group, j] = c

    def pair(which):
        return pl.ds(pl.multiple_of(which * 2 * VD, 2 * VD), 2 * VD)

    def unit(which):
        src, dst = ((k_ref, kk.at[2 + x]), (q_ref, qx.at[x]), (v_ref, vv.at[2 + x]))[which]
        return remote(
            src.at[:, pair(1 - x)], dst, a_send.at[which], a_recv.at[which], beside, tp
        )

    def own_up(which):
        src, dst = ((k_ref, kk), (v_ref, vv))[which]
        return remote(
            src.at[:, pair(x)],
            dst.at[x],
            kv_send.at[which, x],
            kv_recv.at[which, x],
            me + 2,
            tp,
        )

    def other_up(which):
        buf = (kk, vv)[which]
        return remote(
            buf.at[3 - x],
            buf.at[1 - x],
            kv_send.at[which, 1 - x],
            kv_recv.at[which, 1 - x],
            me + 2,
            tp,
        )

    def from_below(which, b):
        buf = (kk, vv)[which]
        return remote(
            buf.at[b], buf.at[b], kv_send.at[which, b], kv_recv.at[which, b], me - 2, tp
        )

    def own_q():
        return remote(
            q_ref.at[:, pair(x)],
            qm.at[high, x],
            qm_send.at[high, x],
            qm_recv.at[high, x],
            hub,
            tp,
        )

    def other_q():
        return remote(
            qx.at[1 - x],
            qm.at[high, 1 - x],
            qm_send.at[high, 1 - x],
            qm_recv.at[high, 1 - x],
            hub,
            tp,
        )

    def q_came(late, b):
        return remote(
            qm.at[late, b],
            qm.at[late, b],
            qm_send.at[late, b],
            qm_recv.at[late, b],
            g + 2 * late + x,
            tp,
        )

    y_copies, core_copies, more_copies = {}, {}, {}

    def hand(group, j):
        s = ahead(j)
        if j == 0:
            src = tok.at[group, w]
            arr[tp, group, w] = tok[group, w]
        else:
            tok_copies[group, j].wait_recv()
            src = arr.at[tp, group, s]
        c = remote(
            src, arr.at[tp, group, s], ty_send.at[group, j], ty_recv.at[group, j], me, tp_y
        )
        c.start()
        y_copies[group, j] = c
        c = remote(
            src,
            arr.at[tp, group, s],
            tc_send.at[0, group, j],
            tc_recv.at[0, group, j],
            me,
            tp_core,
        )
        c.start()
        core_copies[group, j] = c

    scatter(0)

    @pl.when(half == 1)
    def _():
        unit(1).start()

    unit(0).start()
    hand(0, 0)
    kk[2 + x] = k_ref[:, pair(x)]
    qx[x] = q_ref[:, pair(x)]
    vv[2 + x] = v_ref[:, pair(x)]
    for j in (3, 1, 2):
        hand(0, j)
    for c in mirrored:
        c.wait_recv()
    choose(1, routes_m, dense_m)
    scatter(1)
    hand(1, 0)
    unit(2).start()

    @pl.when(half == 0)
    def _():
        unit(1).start()

    @pl.when(half == 1)
    def _():
        own_q().start()
        unit(1).wait_recv()
        other_q().start()

    @pl.when(high == 0)
    def _():
        own_up(0).start()
        unit(0).wait_recv()
        other_up(0).start()
        own_up(1).start()

    def first_products(group, quarter):
        a = arr[quarter, group].reshape(total, width)
        deep = pl.ds(pl.multiple_of(quarter * width, width), width)
        return (
            jnp.dot(a, wg[deep, :], preferred_element_type=jnp.float32),
            jnp.dot(a, wu[deep, :], preferred_element_type=jnp.float32),
        )

    def near_half(group):
        one = first_products(group, tp)
        for j in range(g):
            core_copies[group, j].wait_recv()
        two = first_products(group, tp_core)
        return one[0] + two[0], one[1] + two[1]

    order = (tp_both, tp_y, tp_core, tp)
    near_copies, far_copies = {}, {}

    def far_half(group, gate, up):
        for j in (0, 3, 1, 2):
            s = ahead(j)
            y_copies[group, j].wait_recv()
            c = remote(
                arr.at[tp_y, group, s],
                arr.at[tp_y, group, s],
                tc_send.at[1, group, j],
                tc_recv.at[1, group, j],
                me,
                tp_core,
            )
            c.start()
            more_copies[group, j] = c
        more = first_products(group, tp_y)
        gate, up = gate + more[0], up + more[1]
        for j in range(g):
            more_copies[group, j].wait_recv()
        more = first_products(group, tp_both)
        gate, up = gate + more[0], up + more[1]
        return (jax.nn.silu(gate) * up).astype(jnp.bfloat16)

    def second_products(group, hidden):
        for i in range(4):
            cols = pl.ds(pl.multiple_of(order[i] * width, width), width)
            part[group, i] = (
                jnp.dot(hidden, wd[:, cols], preferred_element_type=jnp.float32)
                .astype(jnp.bfloat16)
                .reshape(g, slots, width)
            )
            if i % 2 == 0:
                h = i // 2
                c = remote(
                    part.at[group, i],
                    near.at[group, h],
                    rc_send.at[group, h],
                    rc_recv.at[group, h],
                    me,
                    tp_core,
                )
                c.start()
                near_copies[group, h] = c
        near_copies[group, 0].wait_recv()
        for c in range(2):
            cols = pl.ds(c * width // 2, width // 2)
            for j in [*range(1, g), 0]:
                d = ahead(j)
                csum[group, d, :, cols] = (
                    part[group, 1, d, :, cols].astype(jnp.float32)
                    + near[group, 0, d, :, cols].astype(jnp.float32)
                ).astype(jnp.bfloat16)
                far_copies[group, c, j] = remote(
                    csum.at[group, d, :, cols],
                    far.at[group, d, :, cols],
                    ry_send.at[group, c, j],
                    ry_recv.at[group, c, j],
                    me,
                    tp_y,
                )
                far_copies[group, c, j].start()

    back_copies = {}

    def expert_back(group, c):
        if c == 0:
            near_copies[group, 1].wait_recv()
        cols = pl.ds(c * width // 2, width // 2)
        for j in [*range(1, g), 0]:
            d = ahead(j)
            far_copies[group, c, j].wait_recv()
            val = (
                part[group, 3, d, :, cols].astype(jnp.float32)
                + near[group, 1, d, :, cols].astype(jnp.float32)
                + far[group, d, :, cols].astype(jnp.float32)
            ).astype(jnp.bfloat16)
            if j == 0:
                ret[group, w, :, cols] = val
            else:
                res[group, d, :, cols] = val
                back_copies[group, c, j] = remote(
                    res.at[group, d, :, cols],
                    ret.at[group, w, :, cols],
                    e_send.at[group, c, j],
                    e_recv.at[group, c, j],
                    base + d,
                    tp,
                )
                back_copies[group, c, j].start()

    def shares_of(ref):
        first, second = upright(ref, 0), upright(ref, 1)
        top = jnp.maximum(first, second)
        raised = (jnp.exp(first - top), jnp.exp(second - top))
        return [raised[k] / (raised[0] + raised[1]) for k in range(TOP)]

    def combine(group, c, gates):
        for j in range(1, g):
            back_copies[group, c, j].wait_recv()
        cols = pl.ds(c * width // 2, width // 2)
        returned = ret[group, :, :, cols].reshape(total, width // 2)
        combined = jnp.zeros((rows_b, width // 2), jnp.float32)
        for k in range(TOP):
            picked = jnp.dot(pick[group, k], returned, preferred_element_type=jnp.float32)
            combined = combined + gates[k] * picked
        return combined

    lam = [lam_ref[x * 2 + h] for h in range(2)]
    size = 2 * rows
    diag = (
        lax.broadcasted_iota(jnp.int32, (size, size), 1)
        <= lax.broadcasted_iota(jnp.int32, (size, size), 0)
    )
    stat_lane = lax.broadcasted_iota(jnp.int32, (size, 128), 1)

    def columns(h, m):
        return slice(h * VD + m * QKD, h * VD + (m + 1) * QKD)

    def weigh(q, first, h, masked):
        found = []
        seen = (4 - first) * rows
        for m in range(2):
            k = kk[first:4].reshape(seen, 2 * VD)[:, columns(h, m)]
            scores = lax.dot_general(
                q[:, columns(h, m)],
                k,
                (((1,), (1,)), ((), ())),
                preferred_element_type=jnp.float32,
            ) * QKD ** (-0.5)
            if masked:
                last = jnp.where(diag, scores[:, seen - size :], neg_big)
                scores = (
                    last
                    if seen == size
                    else jnp.concatenate([scores[:, : seen - size], last], axis=1)
                )
            top = jnp.max(scores, axis=-1, keepdims=True)
            weights = jnp.exp(scores - top)
            found.append((weights, top, jnp.sum(weights, axis=-1, keepdims=True)))
        return found

    def blend(one, two, scale_one, scale_two, first, h):
        v = vv[first:4].reshape((4 - first) * rows, 2 * VD)[:, h * VD : (h + 1) * VD]
        mixed = (one * scale_one - two * scale_two).astype(jnp.bfloat16)
        return jnp.dot(mixed, v, preferred_element_type=jnp.float32)

    def keep(late, place, q, first, masked):
        seen = (4 - first) * rows
        packed = jnp.zeros((size, 128), jnp.float32)
        for h in range(2):
            for m, (weights, top, bottom) in enumerate(weigh(q, first, h, masked)):
                pr[place, h, m, :, 0:seen] = weights
                packed = jnp.where(stat_lane == 4 * h + 2 * m, top, packed)
                packed = jnp.where(stat_lane == 4 * h + 2 * m + 1, bottom, packed)
        stat_out[late] = packed.T[0:8]

    def stats_on(late, to):
        return remote(
            stat_out.at[late], stat_in.at[late], st_send.at[late], st_recv.at[late], to, tp
        )

    def merged(late):
        mine, other = stat_out[late], stat_in[late]
        at = lax.broadcasted_iota(jnp.int32, (128, size), 0)
        table = jnp.zeros((128, size), jnp.float32)
        for h in range(2):
            for m in range(2):
                r = 4 * h + 2 * m
                top, bottom = mine[r : r + 1], mine[r + 1 : r + 2]
                top_o, bottom_o = other[r : r + 1], other[r + 1 : r + 2]
                high_top = jnp.maximum(top, top_o)
                share = jnp.exp(top - high_top)
                scale = share / (bottom * share + bottom_o * jnp.exp(top_o - high_top))
                if m == 1:
                    scale = scale * lam[h]
                table = jnp.where(at == 2 * h + m, scale, table)
        return table.T

    def o_on(late, h, b):
        return remote(
            osend.at[late, h, b],
            oret.at[x, h],
            o_send.at[late, h, b],
            o_recv.at[x, h],
            g + 2 * late + b,
            tp,
        )

    def o_came(side, h):
        return remote(
            oret.at[side, h],
            oret.at[side, h],
            o_send.at[0, h, 0],
            o_recv.at[side, h],
            g // 2 + side,
            tp,
        )

    def f_on(h):
        return remote(fin.at[h, 1 - x], att_in.at[h], f_send.at[h], f_recv.at[h], beside, tp)

    def normal(mixed):
        scaled = mixed * lax.rsqrt(jnp.mean(mixed * mixed, axis=-1, keepdims=True) + head_eps)
        return (scaled * gain_ref[...] * head_scale).astype(jnp.bfloat16)

    def finish(h, mixed):
        fin[h] = normal(mixed).reshape(2, rows, VD)
        f_on(h).start()

    def own_rows():
        return qx[...].reshape(size, 2 * VD)

    def below_came(which):
        for b in range(2):
            from_below(which, b).wait_recv()

    def settle(first):
        for h in range(2):
            one, two = weigh(own_rows(), first, h, True)
            finish(h, blend(one[0], two[0], 1.0 / one[2], lam[h] / two[2], first, h))

    def late_scores(late):
        for b in range(2):
            q_came(late, b).wait_recv()
        keep(late, late, qm[late].reshape(size, 2 * VD), 0, False)
        stats_on(late, g + 2 * late + x).start()

    def late_out(late):
        stats_on(late, g + 2 * late + x).wait_recv()
        scales = merged(late)
        for h in range(2):
            o = blend(
                pr[late, h, 0],
                pr[late, h, 1],
                scales[:, 2 * h : 2 * h + 1],
                scales[:, 2 * h + 1 : 2 * h + 2],
                0,
                h,
            )
            osend[late, h] = o.astype(jnp.bfloat16).reshape(2, rows, VD)
            for b in range(2):
                o_on(late, h, b).start()

    def own_late(late, first):
        seen = (4 - first) * rows
        stats_on(late, hub).wait_recv()
        scales = merged(late)
        for h in range(2):
            o = blend(
                pr[0, h, 0, :, 0:seen],
                pr[0, h, 1, :, 0:seen],
                scales[:, 2 * h : 2 * h + 1],
                scales[:, 2 * h + 1 : 2 * h + 2],
                first,
                h,
            ).reshape(2, rows, VD)
            olate[h] = o
            fin[h] = o.astype(jnp.bfloat16)
            f_on(h).start()

    at_level = [level == i for i in range(4)]

    loads[0].wait()
    loads[1].wait()
    gate, up = near_half(0)
    hidden = far_half(0, gate, up)
    for j in (3, 1, 2):
        hand(1, j)
    loads[2].wait()
    second_products(0, hidden)

    @pl.when(at_level[2])
    def _():
        keep(0, 0, own_rows(), 2, True)
        stats_on(0, hub).start()

    @pl.when(at_level[3])
    def _():
        unit(0).wait_recv()
        below_came(0)
        keep(1, 0, own_rows(), 0, True)
        stats_on(1, hub).start()

    gate, up = near_half(1)

    @pl.when(high == 0)
    def _():
        unit(2).wait_recv()
        other_up(1).start()

    hidden = far_half(1, gate, up)
    second_products(1, hidden)

    @pl.when(at_level[1])
    def _():
        unit(0).wait_recv()
        below_came(0)
        late_scores(0)
        late_scores(1)
        unit(2).wait_recv()
        below_came(1)
        late_out(0)
        late_out(1)

    expert_back(0, 0)
    expert_back(0, 1)

    @pl.when(at_level[0])
    def _():
        unit(1).wait_recv()
        settle(2)

    @pl.when(at_level[2])
    def _():
        own_late(0, 2)

    @pl.when(at_level[3])
    def _():
        unit(2).wait_recv()
        below_came(1)
        own_late(1, 0)

    expert_back(1, 0)
    expert_back(1, 1)

    @pl.when(at_level[1])
    def _():
        unit(1).wait_recv()
        settle(0)

    gates = shares_of(score_m)
    lasts = []
    for c in range(2):
        cols = pl.ds(c * width // 2, width // 2)
        back[:, cols] = combine(1, c, gates).astype(jnp.bfloat16)
        last = remote(
            back.at[:, cols],
            back_m.at[:, cols],
            m_send.at[3 + c],
            m_recv.at[3 + c],
            mirror,
            tp,
        )
        last.start()
        lasts.append(last)
    sent += lasts
    gates = shares_of(score_ref)
    combined = [combine(0, c, gates) for c in range(2)]

    def head_columns(side, h):
        return pl.ds(pl.multiple_of((2 * side + h) * VD, VD), VD)

    @pl.when(half == 1)
    def _():
        for h in range(2):
            o_came(x, h).wait_recv()
            att_ref[:, head_columns(x, h)] = normal(
                olate[h, x] + oret[x, h].astype(jnp.float32)
            )
        for h in range(2):
            f_on(h).wait()
            o_came(1 - x, h).wait_recv()
            att_ref[:, head_columns(1 - x, h)] = normal(
                att_in[h].astype(jnp.float32) + oret[1 - x, h].astype(jnp.float32)
            )

    @pl.when(half == 0)
    def _():
        for h in range(2):
            att_ref[:, head_columns(x, h)] = fin[h, x]
        for h in range(2):
            f_on(h).wait()
            att_ref[:, head_columns(1 - x, h)] = att_in[h]

    for c in range(2):
        cols = pl.ds(c * width // 2, width // 2)
        lasts[c].wait_recv()
        out_ref[:, cols] = (combined[c] + back_m[:, cols].astype(jnp.float32)).astype(
            jnp.bfloat16
        )

    @pl.when(half == 1)
    def _():
        own_q().wait_send()
        other_q().wait_send()
        stats_on(high, hub).wait_send()

    @pl.when(high == 0)
    def _():
        for which in range(2):
            own_up(which).wait_send()
            other_up(which).wait_send()

    @pl.when(at_level[1])
    def _():
        for late in range(2):
            stats_on(late, g + 2 * late + x).wait_send()
            for h in range(2):
                for b in range(2):
                    o_on(late, h, b).wait_send()

    for group in (
        tok_copies,
        y_copies,
        core_copies,
        more_copies,
        near_copies,
        far_copies,
        back_copies,
    ):
        sent += list(group.values())
    for c in sent:
        c.wait_send()
    for which in range(3):
        unit(which).wait_send()


def local(
    queries,
    key_rows,
    values,
    lambdas,
    head_gain,
    tokens,
    moe_gain,
    routes,
    route_scores,
    w_gate,
    w_up,
    w_down,
):
    n = lax.axis_size("ep")
    heads = lambdas.shape[0]
    rows = queries.shape[0]
    rows_b, model = tokens.shape
    slots = 2 * TOP * rows_b // n
    width = model // 4
    ff = w_gate.shape[2]
    vmem = pl.BlockSpec(memory_space=pltpu.VMEM)
    hbm = pl.BlockSpec(memory_space=pl.ANY)
    bf16, f32 = jnp.bfloat16, jnp.float32
    g = n // 2
    dma = pltpu.SemaphoreType.DMA
    shapes = (
        jax.ShapeDtypeStruct(queries.shape, bf16),
        jax.ShapeDtypeStruct((rows_b, width), bf16),
    )
    inside = (pltpu.VMEM(queries.shape, bf16), pltpu.VMEM((rows_b, width), bf16))
    held = pl.pallas_call(
        functools.partial(step_kernel, n, heads),
        out_shape=inside,
        in_specs=[hbm] * 12,
        out_specs=(vmem, vmem),
        scratch_shapes=[
            pltpu.VMEM((model, ff), bf16),
            pltpu.VMEM((model, ff), bf16),
            pltpu.VMEM((ff, model), bf16),
            pltpu.VMEM((2, rows, 2 * VD), bf16),
            pltpu.VMEM((4, rows, 2 * VD), bf16),
            pltpu.VMEM((4, rows, 2 * VD), bf16),
            pltpu.VMEM((2, 2, rows, 2 * VD), bf16),
            pltpu.VMEM((2, 2, 2, 2 * rows, 4 * rows), f32),
            pltpu.VMEM((2, 8, 2 * rows), f32),
            pltpu.VMEM((2, 8, 2 * rows), f32),
            pltpu.VMEM((2, 2, 2, rows, VD), bf16),
            pltpu.VMEM((2, 2, rows, VD), bf16),
            pltpu.VMEM((2, 2, rows, VD), f32),
            pltpu.VMEM((2, 2, rows, VD), bf16),
            pltpu.VMEM((2, rows, VD), bf16),
            pltpu.VMEM((TOP, rows_b), jnp.int32),
            pltpu.VMEM((TOP, rows_b), f32),
            pltpu.VMEM((rows_b, width), bf16),
            pltpu.VMEM((rows_b, width), bf16),
            pltpu.VMEM((2, TOP, rows_b, g * slots), bf16),
            pltpu.VMEM((2, g, slots, width), bf16),
            pltpu.VMEM((4, 2, g, slots, width), bf16),
            pltpu.VMEM((2, 4, g, slots, width), bf16),
            pltpu.VMEM((2, 2, g, slots, width), bf16),
            pltpu.VMEM((2, g, slots, width), bf16),
            pltpu.VMEM((2, g, slots, width), bf16),
            pltpu.VMEM((2, g, slots, width), bf16),
            pltpu.VMEM((2, g, slots, width), bf16),
            pltpu.VMEM((rows_b, width), bf16),
            pltpu.VMEM((rows_b, width), bf16),
            pltpu.VMEM(queries.shape, bf16),
            pltpu.VMEM(queries.shape, bf16),
            pltpu.VMEM(queries.shape, bf16),
            pltpu.VMEM(tokens.shape, bf16),
            pltpu.SMEM(lambdas.shape, f32),
            pltpu.VMEM((1, VD), f32),
            pltpu.VMEM((1, model), f32),
            pltpu.VMEM((TOP, rows_b), jnp.int32),
            pltpu.VMEM((TOP, rows_b), f32),
            dma((12,)),
            dma((5,)),
            dma((5,)),
            dma((2, g)),
            dma((2, g)),
            dma((2, g)),
            dma((2, g)),
            dma((2, 2, g)),
            dma((2, 2, g)),
            dma((3,)),
            dma((3,)),
            dma((2, 2)),
            dma((2, 2)),
            dma((2, 2)),
            dma((2, 2)),
            dma((2,)),
            dma((2,)),
            dma((2, 2, 2)),
            dma((2, 2)),
            dma((2,)),
            dma((2,)),
            dma((2, 2)),
            dma((2, 2)),
            dma((2, 2, g)),
            dma((2, 2, g)),
            dma((2, 2, g)),
            dma((2, 2, g)),
        ],
        compiler_params=pltpu.CompilerParams(
            collective_id=0, has_side_effects=True, vmem_limit_bytes=56 * 1024 * 1024
        ),
    )(
        queries,
        key_rows,
        values,
        lambdas,
        head_gain[None, :],
        tokens,
        moe_gain[None, :],
        routes.T,
        route_scores.T,
        w_gate,
        w_up,
        w_down,
    )
    return tuple(held)


def fits(mesh, head_count):
    n, parts = mesh.shape["ep"], mesh.shape["tp"]
    return parts == 4 and n == 2 * parts and head_count == parts * parts


def solution(mesh):
    def step(*args):
        body = local if fits(mesh, args[3].shape[0]) else local_general
        return sharded(mesh, body)(*args)

    return step


def sharded(mesh, body):
    return jax.shard_map(
        body,
        mesh=mesh,
        in_specs=(
            P("ep", "tp"),
            P("ep", "tp"),
            P("ep", "tp"),
            P("tp"),
            P(),
            P("ep", None),
            P(),
            P("ep", None),
            P("ep", None),
            P("ep", None, "tp"),
            P("ep", None, "tp"),
            P("ep", "tp", None),
        ),
        out_specs=(P("ep", "tp"), P("ep", "tp")),
        check_vma=False,
    )
```
